128 devices in a mesh: sp: 16 (over z, x), tp: 8 (over y, core).
Axes of the slice: x: 4, y: 4, z: 4, core: 2. Of those that a mesh axis runs over, the one named last changes fastest.
Arguments:
- tokens: bfloat16 [4096, 3072], P('sp', 'tp'), may hold values from -6 to 6
- norm_gain: float32 [3072], replicated, may hold values from 0.1 to 1.9
- state_in_weight: bfloat16 [3072, 1024], P('sp', 'tp'), may hold values from -0.109375 to 0.109375
- pool_in_weight: bfloat16 [3072, 1024], P('sp', 'tp'), may hold values from -0.109375 to 0.109375
- rate_real: float32 [64, 64], replicated, may hold values from -1.5 to -0.5
- rate_imag: float32 [64, 64], replicated, may hold values from 0 to 200
- log_step: float32 [64], replicated, may hold values from -2 to 0.7
- input_real: float32 [64, 64, 16], replicated, may hold values from -1 to 1
- input_imag: float32 [64, 64, 16], replicated, may hold values from -1 to 1
- output_real: float32 [64, 16, 64], replicated, may hold values from -112 to 112
- output_imag: float32 [64, 16, 64], replicated, may hold values from -112 to 112
- skip_gain: float32 [1024], replicated, may hold values from -3 to 3
- pool_weight: bfloat16 [16, 64, 64], replicated, may hold values from -0.75 to 0.75
- pool_gain: float32 [1024], replicated, may hold values from 0.1 to 1.9
- state_out_weight: bfloat16 [1024, 3072], P('sp', 'tp'), may hold values from -0.125 to 0.125
- pool_out_weight: bfloat16 [1024, 3072], P('sp', 'tp'), may hold values from -0.125 to 0.125
Outputs:
- mixer_output: bfloat16 [4096, 3072], P('sp', 'tp')
The draws below stay inside these ranges and needn't reach their ends.
All inputs are finite; a program needn't handle non-finite values.
Results may differ from the reference program's by a relative error of at most 0.0065.
Values may be sent and summed in bfloat16 or wider, within the bound.
A program may use at most 64 MiB of HBM per device.

```python
import jax
import jax.numpy as jnp
from jax import lax

D = 3072
SSM_GROUP = 16
SSM_GROUPS = 64
SSM_STATE = 64
POOL_GROUP = 64
POOL_GROUPS = 16
TOKENS = 4096
D_SSM = 1024
D_POOL = 1024


def level_of(key, dims, cuts, smallest, largest):
    gain, own = 1.0, jax.random.fold_in(key, 6)
    for axis_at, shards_of in cuts:
        draws = jnp.exp(jax.random.uniform(jax.random.fold_in(own, axis_at), (shards_of,), jnp.float32, smallest / len(cuts), largest / len(cuts)))
        gain = gain * jnp.repeat(draws, dims[axis_at] // shards_of).reshape([-1 if axis == axis_at else 1 for axis in range(len(dims))])
    return gain


def normal_values(rng, extent, scale, limit, split=(), held_as=jnp.bfloat16):
    array = scale * jax.random.normal(rng, extent, jnp.float32)
    if split:
        array = array * level_of(rng, extent, split, -0.22, 0.18)
    return jnp.clip(array, -limit, limit).astype(held_as)


def setup_inputs(seed: int = 0) -> dict:
    streams_of = jax.random.split(jax.random.key(seed), 17)
    return {
        "tokens": normal_values(streams_of[0], (TOKENS, D), 1.0, 6.0, ((0, 16), (1, 8))),
        "norm_gain": jnp.clip(1.0 + 0.18 * jax.random.normal(streams_of[1], (D,), jnp.float32), 0.1, 1.9),
        "state_in_weight": normal_values(streams_of[2], (D, D_SSM), D ** -0.5, 0.109375, ((0, 16), (1, 8))),
        "pool_in_weight": normal_values(streams_of[3], (D, D_POOL), D ** -0.5, 0.109375, ((0, 16), (1, 8))),
        "rate_real": jnp.clip(jax.random.uniform(streams_of[4], (SSM_GROUPS, SSM_STATE), jnp.float32, -1.5, -0.5), -1.5, -0.5),
        "rate_imag": jnp.clip(jax.random.uniform(streams_of[5], (SSM_GROUPS, SSM_STATE), jnp.float32, 0.0, 200.0), 0.0, 200.0),
        "log_step": jnp.clip(jax.random.uniform(streams_of[6], (SSM_GROUPS,), jnp.float32, -2.0, 0.7), -2.0, 0.7),
        "input_real": normal_values(streams_of[7], (SSM_GROUPS, SSM_STATE, SSM_GROUP), (2 * SSM_GROUP) ** -0.5, 1.0, (), jnp.float32),
        "input_imag": normal_values(streams_of[8], (SSM_GROUPS, SSM_STATE, SSM_GROUP), (2 * SSM_GROUP) ** -0.5, 1.0, (), jnp.float32),
        "output_real": normal_values(streams_of[9], (SSM_GROUPS, SSM_GROUP, SSM_STATE), (TOKENS // 256 + 2), 112.0, (), jnp.float32),
        "output_imag": normal_values(streams_of[10], (SSM_GROUPS, SSM_GROUP, SSM_STATE), (TOKENS // 256 + 2), 112.0, (), jnp.float32),
        "skip_gain": normal_values(streams_of[11], (D_SSM,), 0.5, 3.0, (), jnp.float32),
        "pool_weight": normal_values(streams_of[12], (POOL_GROUPS, POOL_GROUP, POOL_GROUP), POOL_GROUP ** -0.5, 0.75),
        "pool_gain": jnp.clip(1.0 + 0.18 * jax.random.normal(streams_of[13], (D_POOL,), jnp.float32), 0.1, 1.9),
        "state_out_weight": normal_values(streams_of[14], (D_SSM, D), (D_SSM + D_POOL) ** -0.5, 0.125, ((0, 16), (1, 8))),
        "pool_out_weight": normal_values(streams_of[15], (D_POOL, D), (D_SSM + D_POOL) ** -0.5, 0.125, ((0, 16), (1, 8))),
    }


epsilon = 1e-06
highest = lax.Precision.HIGHEST

def discretize(rate_real, rate_imag, log_step, length):
    step_size = jnp.exp(log_step)[:, None] / length
    exponent = rate_real * step_size
    angle = rate_imag * step_size
    magnitude = jnp.exp(exponent)
    decay_real = magnitude * jnp.cos(angle)
    decay_imag = magnitude * jnp.sin(angle)
    less_one = jnp.expm1(exponent) * jnp.cos(angle) - 2.0 * jnp.square(jnp.sin(0.5 * angle))
    denominator = rate_real * rate_real + rate_imag * rate_imag
    factor_real = (less_one * rate_real + decay_imag * rate_imag) / denominator
    factor_imag = (decay_imag * rate_real - less_one * rate_imag) / denominator
    return (exponent, angle, decay_real, decay_imag, factor_real, factor_imag)

def drive_terms(signal, factor_real, factor_imag, input_real, input_imag):
    drive_real = factor_real[..., None] * input_real - factor_imag[..., None] * input_imag
    drive_imag = factor_real[..., None] * input_imag + factor_imag[..., None] * input_real
    push_real = jnp.einsum('tgc,gnc->tgn', signal, drive_real, precision=highest)
    push_imag = jnp.einsum('tgc,gnc->tgn', signal, drive_imag, precision=highest)
    return (push_real, push_imag)

def readout(states_real, states_imag, output_real, output_imag, signal, skip_gain):
    row_count = states_real.shape[0]
    readout_sum = jnp.einsum('tgn,gcn->tgc', states_real, output_real, precision=highest)
    readout_sum = readout_sum - jnp.einsum('tgn,gcn->tgc', states_imag, output_imag, precision=highest)
    readout_sum = readout_sum.reshape(row_count, -1) + skip_gain * signal.reshape(row_count, -1)
    return jax.nn.gelu(readout_sum).astype(jnp.bfloat16)

def pool_mixer(pool_in, pool_weight, pool_gain):
    row_count = pool_in.shape[0]
    signal = pool_in.astype(jnp.float32).reshape(row_count, POOL_GROUPS, POOL_GROUP)
    running = jnp.cumsum(signal, axis=0)
    padded = jnp.pad(running, ((16, 0), (0, 0), (0, 0)))
    positions = jnp.arange(1, row_count + 1)
    window_means = []
    for group_index in range(POOL_GROUPS):
        window = 2 ** (group_index % 4 + 1)
        lagged = padded[16 - window:16 - window + row_count, group_index]
        divisor = jnp.minimum(positions, window).astype(jnp.float32)[:, None]
        window_means.append((running[:, group_index] - lagged) / divisor)
    pooled = jnp.stack(window_means, axis=1) - signal
    projected = jnp.einsum('tgc,gcd->tgd', pooled, pool_weight.astype(jnp.float32), precision=highest)
    return (projected.reshape(row_count, -1) * pool_gain).astype(jnp.bfloat16)

def reference(tokens, norm_gain, state_in_weight, pool_in_weight, rate_real, rate_imag, log_step, input_real, input_imag, output_real, output_imag, skip_gain, pool_weight, pool_gain, state_out_weight, pool_out_weight):
    features = tokens.astype(jnp.float32)
    inverse = lax.rsqrt(lax.optimization_barrier(jnp.sum(features * features, axis=1)) / D + epsilon)[:, None]
    scaled = (features * norm_gain).astype(jnp.bfloat16)
    state_in = (jnp.dot(scaled, state_in_weight, preferred_element_type=jnp.float32) * inverse).astype(jnp.bfloat16)
    pool_in = (jnp.dot(scaled, pool_in_weight, preferred_element_type=jnp.float32) * inverse).astype(jnp.bfloat16)
    signal = state_in.astype(jnp.float32).reshape(TOKENS, SSM_GROUPS, SSM_GROUP)
    exponent, angle, decay_real, decay_imag, factor_real, factor_imag = discretize(rate_real, rate_imag, log_step, TOKENS)
    push_real, push_imag = drive_terms(signal, factor_real, factor_imag, input_real, input_imag)

    def advance(carry, pushes):
        state_real, state_imag = carry
        next_real = decay_real * state_real - decay_imag * state_imag + pushes[0]
        next_imag = decay_real * state_imag + decay_imag * state_real + pushes[1]
        return ((next_real, next_imag), (next_real, next_imag))
    zero_state = jnp.zeros((SSM_GROUPS, SSM_STATE), jnp.float32)
    _, (states_real, states_imag) = lax.scan(advance, (zero_state, zero_state), (push_real, push_imag))
    state_out = readout(states_real, states_imag, output_real, output_imag, signal, skip_gain)
    pool_out = pool_mixer(pool_in, pool_weight, pool_gain)
    combined = jnp.dot(state_out, state_out_weight, preferred_element_type=jnp.float32)
    combined = combined + jnp.dot(pool_out, pool_out_weight, preferred_element_type=jnp.float32)
    return combined.astype(jnp.bfloat16)
```

```python
import functools

import jax
import jax.numpy as jnp
from jax import lax
from jax.experimental import pallas as pl
from jax.experimental.pallas import tpu as pltpu
from jax.sharding import PartitionSpec as P

EPSILON = 1e-06
HIGHEST = lax.Precision.HIGHEST
MESH = pl.DeviceIdType.MESH
F32, BF16 = jnp.float32, jnp.bfloat16

ROWS = 256
STEPS, PARTS = 32, 8
FEATURES = 384
PEERS, HEADS_TP = 16, 8
GROUPS, STATE, CHANNEL = 8, 64, 16
WIDTH = GROUPS * STATE
REACH = 16


def iota(shape, dim):
    return lax.broadcasted_iota(jnp.int32, shape, dim)


def position_of(row):
    return STEPS * (row % PARTS) + row // PARTS


def dot(a, b, precision=None):
    return jnp.dot(a, b, preferred_element_type=F32, precision=precision)


def split(value):
    high = value.astype(BF16)
    return high, (value - high.astype(F32)).astype(BF16)


class Move:
    def __init__(self, sends, fills, device, sems, index):
        self.sends, self.fills, self.device, self.sems, self.index = sends, fills, device, sems, index

    def _copy(self, ref):
        return pltpu.make_async_remote_copy(
            src_ref=ref, dst_ref=ref, send_sem=self.sems[0].at[self.index], recv_sem=self.sems[1].at[self.index],
            device_id=self.device, device_id_type=MESH)

    def start(self):
        self._copy(self.sends).start()

    def arrive(self):
        self._copy(self.fills).wait_recv()

    def left(self):
        self._copy(self.sends).wait_send()


class LineGather:
    def __init__(self, slot, sems, first, y, c):
        d = 1 - 2 * c
        at = lambda k, core: slot(lax.rem(y + k + 4, 4) * 2 + core)
        to = lambda k, core: {"tp": lax.rem(y + k + 4, 4) * 2 + core}
        o = 1 - c
        mk = lambda s, f, dev, i: Move(s, f, dev, sems, first + i)
        self.ahead = mk(at(0, c), at(-d, c), to(d, c), 0)
        self.back = mk(at(0, c), at(d, c), to(-d, c), 1)
        self.onward = mk(at(-d, c), at(-2 * d, c), to(d, c), 2)
        self.own = mk(at(0, c), at(0, o), to(0, o), 3)
        self.cross_ahead = mk(at(-d, c), at(d, o), to(0, o), 4)
        self.cross_back = mk(at(d, c), at(-d, o), to(0, o), 5)
        self.cross_far = mk(at(-2 * d, c), at(2 * d, o), to(0, o), 6)
        self.all = [self.ahead, self.back, self.onward, self.own, self.cross_ahead, self.cross_back, self.cross_far]
        index = lambda k, core: lax.rem(y + k + 4, 4) * 2 + core
        self.index = dict(own=index(0, c), ahead=index(-d, c), back=index(d, c), onward=index(-2 * d, c),
                          p_own=index(0, o), p_ahead=index(d, o), p_back=index(-d, o), p_onward=index(2 * d, o))


class PlaneGather:
    def __init__(self, slot_a, slot_b, sems, first, z, x):
        wrap = lambda k: lax.rem(k + 4, 4)
        at = lambda dz, dx: wrap(z + dz) * 4 + wrap(x + dx)
        self.count = 0

        def mk(slot, sent, filled, device):
            move = Move(slot(at(*sent)), slot(at(*filled)), {"sp": at(*device)}, sems, first + self.count)
            self.count += 1
            return move

        def ring(slot, along, e, base):
            v = (lambda k: (base, k)) if along == "x" else (lambda k: (k, base))
            w = (lambda k: (0, k)) if along == "x" else (lambda k: (k, 0))
            return [
                mk(slot, v(0), v(-e), w(e)),
                mk(slot, v(0), v(e), w(-e)),
                mk(slot, v(-e), v(-2 * e), w(e)),
            ]

        self.a = ring(slot_a, "x", 1, 0)
        self.b = ring(slot_b, "z", -1, 0)
        heavy = {0: 1, -1: 1, 1: -1, 2: -1}
        self.za = {o: ring(slot_a, "z", heavy[o], o) for o in (0, -1, 1, 2)}
        self.xb = {o: ring(slot_b, "x", -heavy[o], o) for o in (0, -1, 1, 2)}
        self.all = [*self.a, *self.b, *(m for r in self.za.values() for m in r), *(m for r in self.xb.values() for m in r)]

    def begin(self):
        for m in (self.a[0], self.a[1], self.b[0], self.b[1], self.za[0][0], self.za[0][1], self.xb[0][0], self.xb[0][1]):
            m.start()

    def events(self):
        def first_of(move, more, ring):
            def event():
                move.arrive()
                if more is not None:
                    more.start()
                ring[0].start()
                ring[1].start()
            return event

        def onward(ring):
            def event():
                ring[0].arrive()
                ring[2].start()
            return event

        def rest():
            for rings in (self.za, self.xb):
                for o in (0, -1, 1, 2):
                    rings[o][1].arrive()
                    rings[o][2].arrive()

        return [
            first_of(self.a[0], self.a[2], self.za[-1]), first_of(self.b[0], self.b[2], self.xb[1]),
            first_of(self.a[1], None, self.za[1]), first_of(self.b[1], None, self.xb[-1]),
            onward(self.za[0]), onward(self.xb[0]),
            first_of(self.a[2], None, self.za[2]), first_of(self.b[2], None, self.xb[2]),
            onward(self.za[-1]), onward(self.xb[1]), onward(self.za[1]), onward(self.xb[-1]),
            onward(self.za[2]), onward(self.xb[2]), rest,
        ]


def kernel(
    tokens, gain_all, state_in_w, pool_in_w, rate_real_all, rate_imag_all, log_step_all, input_real, input_imag,
    output_real, output_imag, skip_all, pool_weight, pool_gain_all, state_out_w, pool_out_w, out,
    gain, rate_real, rate_imag, log_step, skip_gain, pool_gain, own_tokens, tok, scaled, win, wst, wpo, in_re, in_im, out_re, out_im, mix_raw,
    drive, read, unsort, bands, tails, recip, push, high, low, ends, halo, sbuf, pbuf,
    local_sem, tok_send, tok_recv, win_send, win_recv, wout_send, wout_recv,
    end_send, end_recv, halo_send, halo_recv, s_send, s_recv, p_send, p_recv,
):
    s, t = lax.axis_index("sp"), lax.axis_index("tp")
    z, x, y, c = s // 4, s % 4, t // 2, t % 2
    g0 = t * GROUPS

    def lanes(ref, index, width):
        return ref.at[:, pl.ds(pl.multiple_of(index * width, 128), width)]

    def rows(ref, start, count):
        return ref.at[pl.ds(pl.multiple_of(start, 16), count), :]

    loads = [
        (tokens, own_tokens),
        (state_in_w, win.at[pl.ds(pl.multiple_of(s * 192, 16), 192), 0:128]),
        (pool_in_w, win.at[pl.ds(pl.multiple_of(s * 192, 16), 192), 128:256]),
        (state_out_w, rows(wst, s * 64, 64)),
        (pool_out_w, rows(wpo, s * 64, 64)),
        (input_real.at[pl.ds(g0, GROUPS)], in_re),
        (input_imag.at[pl.ds(g0, GROUPS)], in_im),
        (output_real.at[pl.ds(g0, GROUPS)], out_re),
        (output_imag.at[pl.ds(g0, GROUPS)], out_im),
        (pool_weight.at[pl.ds(2 * t, 2)], mix_raw),
        (gain_all, gain),
        (rate_real_all.at[pl.ds(pl.multiple_of(g0, 8), GROUPS), :], rate_real),
        (rate_imag_all.at[pl.ds(pl.multiple_of(g0, 8), GROUPS), :], rate_imag),
        (log_step_all, log_step),
        (lanes(skip_all, t, 128), skip_gain),
        (lanes(pool_gain_all, t, 128), pool_gain),
    ]
    loads = [pltpu.make_async_copy(a, b, local_sem.at[k]) for k, (a, b) in enumerate(loads)]
    for load in loads:
        load.start()

    barrier = pltpu.get_barrier_semaphore()
    for k in range(1, PEERS):
        pl.semaphore_signal(barrier, inc=1, device_id={"sp": lax.rem(s + k, PEERS)}, device_id_type=MESH)
    for k in range(1, HEADS_TP):
        pl.semaphore_signal(barrier, inc=1, device_id={"tp": lax.rem(t + k, HEADS_TP)}, device_id_type=MESH)

    r0, r1 = iota((ROWS, ROWS), 0), iota((ROWS, ROWS), 1)
    loads[0].wait()
    sort = (position_of(r0) == r1).astype(BF16)
    lanes(tok, t, FEATURES)[...] = dot(sort, own_tokens[...]).astype(BF16)
    unsort[...] = (position_of(r1) == r0).astype(BF16)

    line = LineGather(lambda p: lanes(tok, p, FEATURES), (tok_send, tok_recv), 0, y, c)
    w_in = PlaneGather(
        lambda q: rows(win, q * 192, 96), lambda q: rows(win, q * 192 + 96, 96), (win_send, win_recv), 0, z, x)
    w_out = PlaneGather(
        lambda q: rows(wst, q * 64, 64), lambda q: rows(wpo, q * 64, 64), (wout_send, wout_recv), 0, z, x)
    for load in loads[1:]:
        load.wait()

    pl.semaphore_wait(barrier, PEERS - 1 + HEADS_TP - 1)
    line.ahead.start()
    line.back.start()
    line.own.start()
    w_in.begin()

    wanted = iota((GROUPS, STATE), 0) + g0
    steps_log = jnp.sum(jnp.where(iota((GROUPS, 64), 1) == wanted, log_step[...], 0.0), axis=1, keepdims=True)
    step = jnp.exp(steps_log) / float(ROWS * PEERS)
    real = rate_real[...]
    imag = rate_imag[...]
    exponent, angle = real * step, imag * step
    magnitude = jnp.exp(exponent)
    cosine, sine, half_sine = jnp.cos(angle), jnp.sin(angle), jnp.sin(0.5 * angle)
    decay_real, decay_imag = magnitude * cosine, magnitude * sine
    less = exponent * (1.0 + exponent * 0.5 * (1.0 + exponent * (1.0 / 3.0) * (1.0 + exponent * 0.25)))
    less = less * cosine - 2.0 * half_sine * half_sine
    denominator = real * real + imag * imag
    factor_real = (less * real + decay_imag * imag) / denominator
    factor_imag = (decay_imag * real - less * imag) / denominator

    spread = (iota((STATE, WIDTH), 1) % STATE == iota((STATE, WIDTH), 0)).astype(F32)
    own_group = iota((GROUPS, WIDTH), 1) // STATE == iota((GROUPS, WIDTH), 0)

    def flat(value):
        return jnp.sum(jnp.where(own_group, dot(value, spread, HIGHEST), 0.0), axis=0, keepdims=True)

    lr, li = flat(decay_real), flat(decay_imag)
    fr, fi = flat(factor_real), flat(factor_imag)

    def times(ar, ai, br, bi):
        return ar * br - ai * bi, ar * bi + ai * br

    pr, pi = lr, li
    for _ in range(5):
        pr, pi = times(pr, pi, pr, pi)
    part_real, part_imag = pr, pi
    for _ in range(3):
        pr, pi = times(pr, pi, pr, pi)
    block_real, block_imag = pr, pi
    sub = iota((PARTS, WIDTH), 0)
    up_real, up_imag = jnp.ones((PARTS, WIDTH), F32), jnp.zeros((PARTS, WIDTH), F32)
    down_real, down_imag = up_real, up_imag
    wr, wi = jnp.ones((1, WIDTH), F32), jnp.zeros((1, WIDTH), F32)
    for k in range(1, PARTS):
        wr, wi = times(wr, wi, part_real, part_imag)
        up_real, up_imag = jnp.where(sub == k, wr, up_real), jnp.where(sub == k, wi, up_imag)
        down_real = jnp.where(sub == PARTS - 1 - k, wr, down_real)
        down_imag = jnp.where(sub == PARTS - 1 - k, wi, down_imag)

    own_read = iota((128, WIDTH), 0) // CHANNEL == iota((128, WIDTH), 1) // STATE
    for k, ref in enumerate((in_re, in_im)):
        wide = jnp.where(own_read, dot(ref[...].reshape(128, STATE), spread, HIGHEST), 0.0)
        top, rest = split(wide)
        drive[0:128, k * WIDTH : (k + 1) * WIDTH] = top
        drive[128:256, k * WIDTH : (k + 1) * WIDTH] = rest
    cr = jnp.where(own_read, dot(out_re[...].reshape(128, STATE), spread, HIGHEST), 0.0)
    ci = jnp.where(own_read, dot(out_im[...].reshape(128, STATE), spread, HIGHEST), 0.0)
    for k, part in enumerate((cr * fr - ci * fi, -(cr * fi + ci * fr))):
        top, rest = split(jnp.transpose(part))
        read[k * WIDTH : (k + 1) * WIDTH, 0:128] = top
        read[k * WIDTH : (k + 1) * WIDTH, 128:256] = rest

    window0 = jnp.where(c == 0, 2, 8)
    p0, p1 = position_of(r0), position_of(r1)
    for k in range(2):
        w = window0 * (k + 1)
        bands[k * ROWS : (k + 1) * ROWS, :] = ((p1 <= p0) & (p1 > p0 - w)).astype(BF16)
        h0, h1 = position_of(iota((ROWS, REACH), 0)), iota((ROWS, REACH), 1) - REACH
        tails[k * ROWS : (k + 1) * ROWS, :] = (h1 > h0 - w).astype(BF16)
    first_head = iota((ROWS, 128), 1) < 64
    here = position_of(iota((ROWS, 128), 0)) + s * ROWS + 1
    recip[...] = 1.0 / jnp.minimum(here, jnp.where(first_head, window0, 2 * window0)).astype(F32)
    last = (position_of(iota((REACH, ROWS), 1)) == iota((REACH, ROWS), 0) + (ROWS - REACH)).astype(BF16)

    pair = (iota((64, 128), 1) % 64 == iota((64, 128), 0)).astype(BF16)
    mixer = jnp.where(
        iota((128, 128), 0) // 64 == iota((128, 128), 1) // 64, dot(mix_raw[...].reshape(128, 64), pair), 0.0
    ).astype(BF16)

    def prepare(p, squares):
        ref = lanes(tok, p, FEATURES)
        f = ref[...].astype(F32)
        lanes(scaled, p, FEATURES)[...] = (f * gain[:, pl.ds(pl.multiple_of(p * FEATURES, 128), FEATURES)]).astype(BF16)
        f = f * f
        return squares + (f[:, 0:128] + f[:, 128:256] + f[:, 256:384])

    squares = prepare(t, jnp.zeros((ROWS, 128), F32))

    events = w_in.events()
    for e in events[0:4]:
        e()
    line.ahead.arrive()
    line.onward.start()
    line.cross_ahead.start()
    line.back.arrive()
    line.cross_back.start()
    for e in events[4:8]:
        e()
    line.own.arrive()
    squares = prepare(line.index["p_own"], squares)
    squares = prepare(line.index["ahead"], squares)
    squares = prepare(line.index["back"], squares)
    line.onward.arrive()
    line.cross_far.start()
    for e in events[8:14]:
        e()
    w_out.begin()
    for move, name in ((line.cross_ahead, "p_ahead"), (line.cross_back, "p_back")):
        move.arrive()
        squares = prepare(line.index[name], squares)
    squares = prepare(line.index["onward"], squares)
    line.cross_far.arrive()
    squares = prepare(line.index["p_onward"], squares)
    inverse = lax.rsqrt(jnp.sum(squares, axis=1, keepdims=True) / 3072.0 + EPSILON)
    events[14]()

    later = w_out.events()
    for e in later[0:4]:
        e()

    entry = (dot(scaled[...], win[...]) * inverse).astype(BF16)
    state_in, pool_in = entry[:, 0:128], entry[:, 128:256]

    push[...] = dot(jnp.concatenate([state_in, state_in], axis=1), drive[...])
    lrb, lib = jnp.broadcast_to(lr, (PARTS, WIDTH)), jnp.broadcast_to(li, (PARTS, WIDTH))

    def advance(j, carry):
        sr, si = carry
        at = pl.ds(pl.multiple_of(j * PARTS, PARTS), PARTS)
        nr = lrb * sr - lib * si + push[at, 0:WIDTH]
        ni = lrb * si + lib * sr + push[at, WIDTH : 2 * WIDTH]
        return nr, ni

    zero = jnp.zeros((PARTS, WIDTH), F32)
    er, ei = lax.fori_loop(0, STEPS, advance, (zero, zero), unroll=8)
    br, bi = times(er, ei, down_real, down_imag)
    br, bi = jnp.sum(br, axis=0, keepdims=True), jnp.sum(bi, axis=0, keepdims=True)
    lines = lambda row: [row[:, 128 * k : 128 * (k + 1)] for k in range(WIDTH // 128)]
    ends[s] = jnp.concatenate(lines(br) + lines(bi), axis=0)
    moves = [
        Move(ends.at[s], ends.at[lax.rem(s - k + PEERS, PEERS)], {"sp": lax.rem(s + k, PEERS)}, (end_send, end_recv), k)
        for k in range(1, PEERS)
    ]
    for m in moves:
        m.start()

    halo[0] = dot(last, pool_in).astype(BF16)
    halo_move = pltpu.make_async_remote_copy(
        src_ref=halo.at[0], dst_ref=halo.at[1], send_sem=halo_send, recv_sem=halo_recv,
        device_id={"sp": lax.rem(s + 1, PEERS)}, device_id_type=MESH)
    halo_move.start()
    for e in later[4:8]:
        e()
    sums = dot(bands[...], pool_in)
    halo_move.wait_recv()
    before = halo[1]
    before = jnp.where(s > 0, before.astype(F32), 0.0).astype(BF16)
    sums = sums + dot(tails[...], before)
    pooled = jnp.where(first_head, sums[0:ROWS], sums[ROWS : 2 * ROWS]) * recip[...] - pool_in.astype(F32)
    top, rest = split(pooled)
    projected = dot(top, mixer) + dot(rest, mixer)
    pool_out = (projected * pool_gain[...]).astype(BF16)
    lanes(pbuf, t, 128)[...] = dot(unsort[...], pool_out).astype(BF16)
    pline = LineGather(lambda p: lanes(pbuf, p, 128), (p_send, p_recv), 0, y, c)
    pline.ahead.start()
    pline.back.start()
    pline.own.start()
    for e in later[8:12]:
        e()

    kr, ki = jnp.where(sub >= 1, pltpu.roll(er, 1, 0), 0.0), jnp.where(sub >= 1, pltpu.roll(ei, 1, 0), 0.0)
    gr, gi = part_real, part_imag
    for hop in (1, 2, 4):
        tr = jnp.where(sub >= hop, pltpu.roll(kr, hop, 0), 0.0)
        ti = jnp.where(sub >= hop, pltpu.roll(ki, hop, 0), 0.0)
        ar, ai = times(tr, ti, gr, gi)
        kr, ki = kr + ar, ki + ai
        gr, gi = times(gr, gi, gr, gi)

    pline.ahead.arrive()
    pline.onward.start()
    pline.cross_ahead.start()
    pline.back.arrive()
    pline.cross_back.start()

    for m in moves:
        m.arrive()
    qr = jnp.concatenate(lines(block_real), axis=0)
    qi = jnp.concatenate(lines(block_imag), axis=0)
    hr, hi = jnp.zeros_like(qr), jnp.zeros_like(qi)
    for q in range(PEERS - 1):
        piece = ends[q]
        ar, ai = times(hr, hi, qr, qi)
        hr, hi = jnp.where(q < s, ar + piece[0:4], hr), jnp.where(q < s, ai + piece[4:8], hi)
    hr = jnp.concatenate([hr[k : k + 1] for k in range(4)], axis=1)
    hi = jnp.concatenate([hi[k : k + 1] for k in range(4)], axis=1)
    ar, ai = times(up_real, up_imag, hr, hi)

    def advance_pair(j, carry):
        one = advance(2 * j, carry)
        two = advance(2 * j + 1, one)
        at = pl.ds(pl.multiple_of(j * 2 * PARTS, 2 * PARTS), 2 * PARTS)
        for k in range(2):
            top, rest = split(jnp.concatenate([one[k], two[k]], axis=0))
            high[at, k * WIDTH : (k + 1) * WIDTH] = top
            low[at, k * WIDTH : (k + 1) * WIDTH] = rest
        return two

    lax.fori_loop(0, STEPS // 2, advance_pair, (kr + ar, ki + ai), unroll=4)
    both = dot(high[...], read[...])
    readout = both[:, 0:128] + both[:, 128:256] + dot(low[...], read[:, 0:128])
    readout = readout + skip_gain[...] * state_in.astype(F32)
    state_out = jax.nn.gelu(readout).astype(BF16)
    lanes(sbuf, t, 128)[...] = dot(unsort[...], state_out).astype(BF16)
    sline = LineGather(lambda p: lanes(sbuf, p, 128), (s_send, s_recv), 0, y, c)
    sline.ahead.start()
    sline.back.start()
    sline.own.start()

    pline.onward.arrive()
    pline.cross_far.start()
    for e in later[12:15]:
        e()
    for m in (pline.own, pline.cross_ahead, pline.cross_back, pline.cross_far):
        m.arrive()
    sline.ahead.arrive()
    sline.onward.start()
    sline.cross_ahead.start()
    sline.back.arrive()
    sline.cross_back.start()
    total = dot(pbuf[...], wpo[...])
    sline.onward.arrive()
    sline.cross_far.start()
    for m in (sline.own, sline.cross_ahead, sline.cross_back, sline.cross_far):
        m.arrive()
    out[...] = (total + dot(sbuf[...], wst[...])).astype(BF16)

    for m in (*line.all, *w_in.all, *w_out.all, *moves, *pline.all, *sline.all):
        m.left()
    halo_move.wait_send()


def body(
    tokens, norm_gain, state_in_weight, pool_in_weight, rate_real, rate_imag, log_step, input_real, input_imag,
    output_real, output_imag, skip_gain, pool_weight, pool_gain, state_out_weight, pool_out_weight,
):
    vmem = pl.BlockSpec(memory_space=pltpu.VMEM)
    dma = pltpu.SemaphoreType.DMA
    return pl.pallas_call(
        kernel,
        out_shape=jax.ShapeDtypeStruct((ROWS, FEATURES), BF16),
        in_specs=[pl.BlockSpec(memory_space=pltpu.HBM)] * 16,
        out_specs=vmem,
        scratch_shapes=[
            pltpu.VMEM((1, 3072), F32),
            pltpu.VMEM((GROUPS, STATE), F32),
            pltpu.VMEM((GROUPS, STATE), F32),
            pltpu.VMEM((1, 64), F32),
            pltpu.VMEM((1, 128), F32),
            pltpu.VMEM((1, 128), F32),
            pltpu.VMEM((ROWS, FEATURES), BF16),
            pltpu.VMEM((ROWS, 3072), BF16),
            pltpu.VMEM((ROWS, 3072), BF16),
            pltpu.VMEM((3072, 256), BF16),
            pltpu.VMEM((1024, FEATURES), BF16),
            pltpu.VMEM((1024, FEATURES), BF16),
            pltpu.VMEM((GROUPS, CHANNEL, STATE), F32),
            pltpu.VMEM((GROUPS, CHANNEL, STATE), F32),
            pltpu.VMEM((GROUPS, CHANNEL, STATE), F32),
            pltpu.VMEM((GROUPS, CHANNEL, STATE), F32),
            pltpu.VMEM((2, 64, 64), BF16),
            pltpu.VMEM((256, 2 * WIDTH), BF16),
            pltpu.VMEM((2 * WIDTH, 256), BF16),
            pltpu.VMEM((ROWS, ROWS), BF16),
            pltpu.VMEM((2 * ROWS, ROWS), BF16),
            pltpu.VMEM((2 * ROWS, REACH), BF16),
            pltpu.VMEM((ROWS, 128), F32),
            pltpu.VMEM((ROWS, 2 * WIDTH), F32),
            pltpu.VMEM((ROWS, 2 * WIDTH), BF16),
            pltpu.VMEM((ROWS, 2 * WIDTH), BF16),
            pltpu.VMEM((PEERS, 8, 128), F32),
            pltpu.VMEM((2, REACH, 128), BF16),
            pltpu.VMEM((ROWS, 1024), BF16),
            pltpu.VMEM((ROWS, 1024), BF16),
            dma((16,)), dma((7,)), dma((7,)), dma((30,)), dma((30,)), dma((30,)), dma((30,)),
            dma((PEERS,)), dma((PEERS,)), dma(()), dma(()), dma((7,)), dma((7,)), dma((7,)), dma((7,)),
        ],
        compiler_params=pltpu.CompilerParams(collective_id=0, has_side_effects=True, vmem_limit_bytes=48 << 20),
    )(
        tokens, norm_gain.reshape(1, 3072), state_in_weight, pool_in_weight, rate_real, rate_imag,
        log_step.reshape(1, 64), jnp.swapaxes(input_real, 1, 2), jnp.swapaxes(input_imag, 1, 2), output_real, output_imag, skip_gain.reshape(1, 1024),
        pool_weight, pool_gain.reshape(1, 1024), state_out_weight, pool_out_weight,
    )


def solution(mesh):
    tile = P("sp", "tp")
    in_specs = (tile, P(), tile, tile, *(P() for _ in range(10)), tile, tile)
    return jax.shard_map(body, mesh=mesh, in_specs=in_specs, out_specs=tile, check_vma=False)
```

```python
import functools

import jax
import jax.numpy as jnp
from jax import lax
from jax.experimental import pallas as pl
from jax.experimental.pallas import tpu as pltpu
from jax.sharding import PartitionSpec as P

EPSILON = 1e-06
HIGHEST = lax.Precision.HIGHEST
MESH = pl.DeviceIdType.MESH
F32, BF16 = jnp.float32, jnp.bfloat16

ROWS = 256
STEPS, PARTS = 32, 8
FEATURES = 384
PEERS, HEADS_TP = 16, 8
GROUPS, STATE, CHANNEL = 8, 64, 16
WIDTH = GROUPS * STATE
REACH = 16


def iota(shape, dim):
    return lax.broadcasted_iota(jnp.int32, shape, dim)


def position_of(row):
    return STEPS * (row % PARTS) + row // PARTS


def dot(a, b, precision=None):
    return jnp.dot(a, b, preferred_element_type=F32, precision=precision)


def split(value):
    high = value.astype(BF16)
    return high, (value - high.astype(F32)).astype(BF16)


class Move:
    def __init__(self, sends, fills, device, sems, index):
        self.sends, self.fills, self.device, self.sems, self.index = sends, fills, device, sems, index

    def _copy(self, ref):
        return pltpu.make_async_remote_copy(
            src_ref=ref, dst_ref=ref, send_sem=self.sems[0].at[self.index], recv_sem=self.sems[1].at[self.index],
            device_id=self.device, device_id_type=MESH)

    def start(self):
        self._copy(self.sends).start()

    def arrive(self):
        self._copy(self.fills).wait_recv()

    def left(self):
        self._copy(self.sends).wait_send()


class LineGather:
    def __init__(self, slot, sems, first, y, c):
        d = 1 - 2 * c
        at = lambda k, core: slot(lax.rem(y + k + 4, 4) * 2 + core)
        to = lambda k, core: {"tp": lax.rem(y + k + 4, 4) * 2 + core}
        o = 1 - c
        mk = lambda s, f, dev, i: Move(s, f, dev, sems, first + i)
        self.ahead = mk(at(0, c), at(-d, c), to(d, c), 0)
        self.back = mk(at(0, c), at(d, c), to(-d, c), 1)
        self.onward = mk(at(-d, c), at(-2 * d, c), to(d, c), 2)
        self.own = mk(at(0, c), at(0, o), to(0, o), 3)
        self.cross_ahead = mk(at(-d, c), at(d, o), to(0, o), 4)
        self.cross_back = mk(at(d, c), at(-d, o), to(0, o), 5)
        self.cross_far = mk(at(-2 * d, c), at(2 * d, o), to(0, o), 6)
        self.all = [self.ahead, self.back, self.onward, self.own, self.cross_ahead, self.cross_back, self.cross_far]
        index = lambda k, core: lax.rem(y + k + 4, 4) * 2 + core
        self.index = dict(own=index(0, c), ahead=index(-d, c), back=index(d, c), onward=index(-2 * d, c),
                          p_own=index(0, o), p_ahead=index(d, o), p_back=index(-d, o), p_onward=index(2 * d, o))


class PlaneGather:
    def __init__(self, slot_a, slot_b, sems, first, z, x):
        wrap = lambda k: lax.rem(k + 4, 4)
        at = lambda dz, dx: wrap(z + dz) * 4 + wrap(x + dx)
        self.count = 0

        def mk(slot, sent, filled, device):
            move = Move(slot(at(*sent)), slot(at(*filled)), {"sp": at(*device)}, sems, first + self.count)
            self.count += 1
            return move

        def ring(slot, along, e, base, far):
            v = (lambda k: (base, k)) if along == "x" else (lambda k: (k, base))
            w = (lambda k: (0, k)) if along == "x" else (lambda k: (k, 0))
            return [
                mk(slot, v(0), v(-e), w(e)),
                mk(slot, v(0), v(e), w(-e)),
                mk(slot, v(0), v(2), w(2)) if far else mk(slot, v(-e), v(-2 * e), w(e)),
            ]

        self.a = ring(slot_a, "x", 1, 0, True)
        self.b = ring(slot_b, "z", -1, 0, True)
        heavy = {0: 1, -1: -1, 1: -1, 2: 1}
        self.za = {o: ring(slot_a, "z", heavy[o], o, o == 2) for o in (0, -1, 1, 2)}
        self.xb = {o: ring(slot_b, "x", -heavy[o], o, o == 2) for o in (0, -1, 1, 2)}
        self.all = [*self.a, *self.b, *(m for r in self.za.values() for m in r), *(m for r in self.xb.values() for m in r)]

    def begin(self):
        for ring in (self.a, self.b):
            ring[0].start()
            ring[1].start()
        for ring in (self.a, self.b):
            ring[2].start()
        for ring in (self.za[0], self.xb[0]):
            ring[0].start()
            ring[1].start()

    def events(self):
        def across(move, ring, count):
            def event():
                move.arrive()
                for k in range(count):
                    ring[k].start()
            return event

        def onward(ring):
            def event():
                ring[0].arrive()
                ring[2].start()
            return event

        def rest():
            for rings in (self.za, self.xb):
                for o in (0, -1, 1):
                    rings[o][1].arrive()
                for o in (0, -1, 1):
                    rings[o][2].arrive()
                for move in rings[2]:
                    move.arrive()

        return [
            across(self.a[0], self.za[-1], 2), across(self.b[0], self.xb[1], 2),
            across(self.a[1], self.za[1], 2), across(self.b[1], self.xb[-1], 2),
            across(self.a[2], self.za[2], 3), across(self.b[2], self.xb[2], 3),
            onward(self.za[0]), onward(self.xb[0]),
            onward(self.za[-1]), onward(self.xb[1]), onward(self.za[1]), onward(self.xb[-1]), rest,
        ]


def kernel(
    tokens, gain_all, state_in_w, pool_in_w, rate_real_all, rate_imag_all, log_step_all, input_real, input_imag,
    output_real, output_imag, skip_all, pool_weight, pool_gain_all, state_out_w, pool_out_w, out,
    gain, rate_real, rate_imag, log_step, skip_gain, pool_gain, own_tokens, tok, scaled, win, wst, wpo, in_re, in_im, out_re, out_im, mix_raw,
    drive, read, unsort, bands, tails, recip, push, high, low, ends, halo, sbuf, pbuf,
    local_sem, tok_send, tok_recv, win_send, win_recv, wout_send, wout_recv,
    ready, end_send, end_recv, halo_send, halo_recv, s_send, s_recv, p_send, p_recv,
):
    s, t = lax.axis_index("sp"), lax.axis_index("tp")
    z, x, y, c = s // 4, s % 4, t // 2, t % 2
    g0 = t * GROUPS

    def lanes(ref, index, width):
        return ref.at[:, pl.ds(pl.multiple_of(index * width, 128), width)]

    def rows(ref, start, count):
        return ref.at[pl.ds(pl.multiple_of(start, 16), count), :]

    loads = [
        (tokens, own_tokens),
        (state_in_w, win.at[pl.ds(pl.multiple_of(s * 192, 16), 192), 0:128]),
        (pool_in_w, win.at[pl.ds(pl.multiple_of(s * 192, 16), 192), 128:256]),
        (state_out_w, rows(wst, s * 64, 64)),
        (pool_out_w, rows(wpo, s * 64, 64)),
        (input_real.at[pl.ds(g0, GROUPS)], in_re),
        (input_imag.at[pl.ds(g0, GROUPS)], in_im),
        (output_real.at[pl.ds(g0, GROUPS)], out_re),
        (output_imag.at[pl.ds(g0, GROUPS)], out_im),
        (pool_weight.at[pl.ds(2 * t, 2)], mix_raw),
        (gain_all, gain),
        (rate_real_all.at[pl.ds(pl.multiple_of(g0, 8), GROUPS), :], rate_real),
        (rate_imag_all.at[pl.ds(pl.multiple_of(g0, 8), GROUPS), :], rate_imag),
        (log_step_all, log_step),
        (lanes(skip_all, t, 128), skip_gain),
        (lanes(pool_gain_all, t, 128), pool_gain),
    ]
    loads = [pltpu.make_async_copy(a, b, local_sem.at[k]) for k, (a, b) in enumerate(loads)]
    for load in loads:
        load.start()

    barrier = pltpu.get_barrier_semaphore()
    beside = [z * 4 + lax.rem(x + k, 4) for k in (1, 2, 3)]
    above = [lax.rem(z + k, 4) * 4 + x for k in (1, 2, 3)]
    for peer in (*beside, *above):
        pl.semaphore_signal(barrier, inc=1, device_id={"sp": peer}, device_id_type=MESH)
    for k in range(1, HEADS_TP):
        pl.semaphore_signal(barrier, inc=1, device_id={"tp": lax.rem(t + k, HEADS_TP)}, device_id_type=MESH)

    r0, r1 = iota((ROWS, ROWS), 0), iota((ROWS, ROWS), 1)
    loads[0].wait()
    sort = (position_of(r0) == r1).astype(BF16)
    lanes(tok, t, FEATURES)[...] = dot(sort, own_tokens[...]).astype(BF16)
    unsort[...] = (position_of(r1) == r0).astype(BF16)

    def halves(ref, width, sems):
        def of(k):
            return lambda p: ref.at[pl.ds(k * 128, 128), pl.ds(pl.multiple_of(p * width, 128), width)]
        return [LineGather(of(k), sems, 7 * k, y, c) for k in range(2)]

    tok_lines = halves(tok, FEATURES, (tok_send, tok_recv))
    w_in = PlaneGather(
        lambda q: rows(win, q * 192, 96), lambda q: rows(win, q * 192 + 96, 96), (win_send, win_recv), 0, z, x)
    w_out = PlaneGather(
        lambda q: rows(wst, q * 64, 64), lambda q: rows(wpo, q * 64, 64), (wout_send, wout_recv), 0, z, x)
    for load in loads[1:3]:
        load.wait()

    pl.semaphore_wait(barrier, 6 + HEADS_TP - 1)
    for line in tok_lines:
        line.ahead.start()
        line.back.start()
    w_in.begin()
    for line in tok_lines:
        line.own.start()
    for peer in beside:
        pl.semaphore_signal(ready, inc=1, device_id={"sp": peer}, device_id_type=MESH)
    for load in loads[3:]:
        load.wait()

    wanted = iota((GROUPS, STATE), 0) + g0
    steps_log = jnp.sum(jnp.where(iota((GROUPS, 64), 1) == wanted, log_step[...], 0.0), axis=1, keepdims=True)
    step = jnp.exp(steps_log) / float(ROWS * PEERS)
    real = rate_real[...]
    imag = rate_imag[...]
    exponent, angle = real * step, imag * step
    magnitude = jnp.exp(exponent)
    cosine, sine, half_sine = jnp.cos(angle), jnp.sin(angle), jnp.sin(0.5 * angle)
    decay_real, decay_imag = magnitude * cosine, magnitude * sine
    less = exponent * (1.0 + exponent * 0.5 * (1.0 + exponent * (1.0 / 3.0) * (1.0 + exponent * 0.25)))
    less = less * cosine - 2.0 * half_sine * half_sine
    denominator = real * real + imag * imag
    factor_real = (less * real + decay_imag * imag) / denominator
    factor_imag = (decay_imag * real - less * imag) / denominator

    spread = (iota((STATE, WIDTH), 1) % STATE == iota((STATE, WIDTH), 0)).astype(F32)
    own_group = iota((GROUPS, WIDTH), 1) // STATE == iota((GROUPS, WIDTH), 0)

    def flat(value):
        return jnp.sum(jnp.where(own_group, dot(value, spread, HIGHEST), 0.0), axis=0, keepdims=True)

    lr, li = flat(decay_real), flat(decay_imag)
    fr, fi = flat(factor_real), flat(factor_imag)

    def times(ar, ai, br, bi):
        return ar * br - ai * bi, ar * bi + ai * br

    pr, pi = lr, li
    for _ in range(5):
        pr, pi = times(pr, pi, pr, pi)
    part_real, part_imag = pr, pi
    for _ in range(3):
        pr, pi = times(pr, pi, pr, pi)
    block_real, block_imag = pr, pi
    sub = iota((PARTS, WIDTH), 0)
    up_real, up_imag = jnp.ones((PARTS, WIDTH), F32), jnp.zeros((PARTS, WIDTH), F32)
    down_real, down_imag = up_real, up_imag
    wr, wi = jnp.ones((1, WIDTH), F32), jnp.zeros((1, WIDTH), F32)
    for k in range(1, PARTS):
        wr, wi = times(wr, wi, part_real, part_imag)
        up_real, up_imag = jnp.where(sub == k, wr, up_real), jnp.where(sub == k, wi, up_imag)
        down_real = jnp.where(sub == PARTS - 1 - k, wr, down_real)
        down_imag = jnp.where(sub == PARTS - 1 - k, wi, down_imag)

    own_read = iota((128, WIDTH), 0) // CHANNEL == iota((128, WIDTH), 1) // STATE
    for k, ref in enumerate((in_re, in_im)):
        wide = jnp.where(own_read, dot(ref[...].reshape(128, STATE), spread, HIGHEST), 0.0)
        top, rest = split(wide)
        drive[0:128, k * WIDTH : (k + 1) * WIDTH] = top
        drive[128:256, k * WIDTH : (k + 1) * WIDTH] = rest
    cr = jnp.where(own_read, dot(out_re[...].reshape(128, STATE), spread, HIGHEST), 0.0)
    ci = jnp.where(own_read, dot(out_im[...].reshape(128, STATE), spread, HIGHEST), 0.0)
    for k, part in enumerate((cr * fr - ci * fi, -(cr * fi + ci * fr))):
        top, rest = split(jnp.transpose(part))
        read[k * WIDTH : (k + 1) * WIDTH, 0:128] = top
        read[k * WIDTH : (k + 1) * WIDTH, 128:256] = rest

    window0 = jnp.where(c == 0, 2, 8)
    p0, p1 = position_of(r0), position_of(r1)
    for k in range(2):
        w = window0 * (k + 1)
        bands[k * ROWS : (k + 1) * ROWS, :] = ((p1 <= p0) & (p1 > p0 - w)).astype(BF16)
        h0, h1 = position_of(iota((ROWS, REACH), 0)), iota((ROWS, REACH), 1) - REACH
        tails[k * ROWS : (k + 1) * ROWS, :] = (h1 > h0 - w).astype(BF16)
    first_head = iota((ROWS, 128), 1) < 64
    here = position_of(iota((ROWS, 128), 0)) + s * ROWS + 1
    recip[...] = 1.0 / jnp.minimum(here, jnp.where(first_head, window0, 2 * window0)).astype(F32)
    last = (position_of(iota((REACH, ROWS), 1)) == iota((REACH, ROWS), 0) + (ROWS - REACH)).astype(BF16)

    pair = (iota((64, 128), 1) % 64 == iota((64, 128), 0)).astype(BF16)
    mixer = jnp.where(
        iota((128, 128), 0) // 64 == iota((128, 128), 1) // 64, dot(mix_raw[...].reshape(128, 64), pair), 0.0
    ).astype(BF16)

    def prepare(p, squares):
        ref = lanes(tok, p, FEATURES)
        f = ref[...].astype(F32)
        lanes(scaled, p, FEATURES)[...] = (f * gain[:, pl.ds(pl.multiple_of(p * FEATURES, 128), FEATURES)]).astype(BF16)
        f = f * f
        return squares + (f[:, 0:128] + f[:, 128:256] + f[:, 256:384])

    squares = prepare(t, jnp.zeros((ROWS, 128), F32))

    def relay(line):
        line.ahead.arrive()
        line.onward.start()
        line.cross_ahead.start()
        line.back.arrive()
        line.cross_back.start()

    def relay_far(line):
        line.onward.arrive()
        line.cross_far.start()

    events = w_in.events()
    one, two = tok_lines
    for e in events[0:4]:
        e()
    relay(one)
    for e in events[4:8]:
        e()
    relay(two)
    index = one.index
    for e in events[8:12]:
        e()
    w_out.begin()
    relay_far(one)
    one.own.arrive()
    two.own.arrive()
    for name in ("p_own", "ahead", "back"):
        squares = prepare(index[name], squares)
    one.cross_ahead.arrive()
    one.cross_back.arrive()
    two.cross_ahead.arrive()
    squares = prepare(index["p_ahead"], squares)
    two.cross_back.arrive()
    squares = prepare(index["p_back"], squares)
    relay_far(two)
    squares = prepare(index["onward"], squares)
    one.cross_far.arrive()
    two.cross_far.arrive()
    squares = prepare(index["p_onward"], squares)
    inverse = lax.rsqrt(jnp.sum(squares, axis=1, keepdims=True) / 3072.0 + EPSILON)
    events[12]()
    later = w_out.events()

    entry = (dot(scaled[...], win[...]) * inverse).astype(BF16)
    state_in, pool_in = entry[:, 0:128], entry[:, 128:256]

    push[...] = dot(jnp.concatenate([state_in, state_in], axis=1), drive[...])
    lrb, lib = jnp.broadcast_to(lr, (PARTS, WIDTH)), jnp.broadcast_to(li, (PARTS, WIDTH))

    def advance(j, carry):
        sr, si = carry
        at = pl.ds(pl.multiple_of(j * PARTS, PARTS), PARTS)
        nr = lrb * sr - lib * si + push[at, 0:WIDTH]
        ni = lrb * si + lib * sr + push[at, WIDTH : 2 * WIDTH]
        return nr, ni

    zero = jnp.zeros((PARTS, WIDTH), F32)
    er, ei = lax.fori_loop(0, STEPS, advance, (zero, zero), unroll=8)
    br, bi = times(er, ei, down_real, down_imag)
    br, bi = jnp.sum(br, axis=0, keepdims=True), jnp.sum(bi, axis=0, keepdims=True)
    lines = lambda row: [row[:, 128 * k : 128 * (k + 1)] for k in range(WIDTH // 128)]
    ends[s] = jnp.concatenate(lines(br) + lines(bi), axis=0)
    moves = [
        Move(ends.at[s], ends.at[lax.rem(s - k + PEERS, PEERS)], {"sp": lax.rem(s + k, PEERS)}, (end_send, end_recv), k)
        for k in range(1, PEERS)
    ]
    pl.semaphore_wait(ready, 3)
    for m in moves:
        m.start()

    halo[s] = dot(last, pool_in).astype(BF16)
    back = lax.rem(s + PEERS - 1, PEERS)
    halo_move = Move(halo.at[s], halo.at[back], {"sp": lax.rem(s + 1, PEERS)}, (halo_send, halo_recv), 0)
    halo_move.start()
    for e in later[0:6]:
        e()
    sums = dot(bands[...], pool_in)
    halo_move.arrive()
    before = halo[back]
    before = jnp.where(s > 0, before.astype(F32), 0.0).astype(BF16)
    sums = sums + dot(tails[...], before)
    pooled = jnp.where(first_head, sums[0:ROWS], sums[ROWS : 2 * ROWS]) * recip[...] - pool_in.astype(F32)
    top, rest = split(pooled)
    projected = dot(top, mixer) + dot(rest, mixer)
    pool_out = (projected * pool_gain[...]).astype(BF16)
    lanes(pbuf, t, 128)[...] = dot(unsort[...], pool_out).astype(BF16)
    pline = LineGather(lambda p: lanes(pbuf, p, 128), (p_send, p_recv), 0, y, c)
    pline.ahead.start()
    pline.back.start()
    pline.own.start()

    kr, ki = jnp.where(sub >= 1, pltpu.roll(er, 1, 0), 0.0), jnp.where(sub >= 1, pltpu.roll(ei, 1, 0), 0.0)
    gr, gi = part_real, part_imag
    for hop in (1, 2, 4):
        tr = jnp.where(sub >= hop, pltpu.roll(kr, hop, 0), 0.0)
        ti = jnp.where(sub >= hop, pltpu.roll(ki, hop, 0), 0.0)
        ar, ai = times(tr, ti, gr, gi)
        kr, ki = kr + ar, ki + ai
        gr, gi = times(gr, gi, gr, gi)

    for e in later[6:12]:
        e()
    for m in moves:
        m.arrive()
    qr = jnp.concatenate(lines(block_real), axis=0)
    qi = jnp.concatenate(lines(block_imag), axis=0)
    hr, hi = jnp.zeros_like(qr), jnp.zeros_like(qi)
    for q in range(PEERS - 1):
        piece = ends[q]
        ar, ai = times(hr, hi, qr, qi)
        hr, hi = jnp.where(q < s, ar + piece[0:4], hr), jnp.where(q < s, ai + piece[4:8], hi)
    hr = jnp.concatenate([hr[k : k + 1] for k in range(4)], axis=1)
    hi = jnp.concatenate([hi[k : k + 1] for k in range(4)], axis=1)
    ar, ai = times(up_real, up_imag, hr, hi)

    def advance_pair(j, carry):
        one = advance(2 * j, carry)
        two = advance(2 * j + 1, one)
        at = pl.ds(pl.multiple_of(j * 2 * PARTS, 2 * PARTS), 2 * PARTS)
        for k in range(2):
            top, rest = split(jnp.concatenate([one[k], two[k]], axis=0))
            high[at, k * WIDTH : (k + 1) * WIDTH] = top
            low[at, k * WIDTH : (k + 1) * WIDTH] = rest
        return two

    lax.fori_loop(0, STEPS // 2, advance_pair, (kr + ar, ki + ai), unroll=4)
    relay(pline)
    both = dot(high[...], read[...])
    readout = both[:, 0:128] + both[:, 128:256] + dot(low[...], read[:, 0:128])
    readout = readout + skip_gain[...] * state_in.astype(F32)
    state_out = jax.nn.gelu(readout).astype(BF16)
    lanes(sbuf, t, 128)[...] = dot(unsort[...], state_out).astype(BF16)
    s_lines = halves(sbuf, 128, (s_send, s_recv))
    for line in s_lines:
        line.ahead.start()
        line.back.start()
    for line in s_lines:
        line.own.start()
    relay_far(pline)
    later[12]()
    for m in (pline.own, pline.cross_ahead, pline.cross_back, pline.cross_far):
        m.arrive()
    total = dot(pbuf[...], wpo[...])
    for line in s_lines:
        relay(line)
    for line in s_lines:
        relay_far(line)
    for line in s_lines:
        for m in (line.own, line.cross_ahead, line.cross_back, line.cross_far):
            m.arrive()
    out[...] = (total + dot(sbuf[...], wst[...])).astype(BF16)

    for m in (*(m for line in (*tok_lines, *s_lines) for m in line.all), *w_in.all, *w_out.all, *moves, *pline.all):
        m.left()
    halo_move.left()


def body(
    tokens, norm_gain, state_in_weight, pool_in_weight, rate_real, rate_imag, log_step, input_real, input_imag,
    output_real, output_imag, skip_gain, pool_weight, pool_gain, state_out_weight, pool_out_weight,
):
    vmem = pl.BlockSpec(memory_space=pltpu.VMEM)
    dma = pltpu.SemaphoreType.DMA
    return pl.pallas_call(
        kernel,
        out_shape=pltpu.VMEM((ROWS, FEATURES), BF16),
        in_specs=[pl.BlockSpec(memory_space=pltpu.HBM)] * 16,
        out_specs=vmem,
        scratch_shapes=[
            pltpu.VMEM((1, 3072), F32),
            pltpu.VMEM((GROUPS, STATE), F32),
            pltpu.VMEM((GROUPS, STATE), F32),
            pltpu.VMEM((1, 64), F32),
            pltpu.VMEM((1, 128), F32),
            pltpu.VMEM((1, 128), F32),
            pltpu.VMEM((ROWS, FEATURES), BF16),
            pltpu.VMEM((ROWS, 3072), BF16),
            pltpu.VMEM((ROWS, 3072), BF16),
            pltpu.VMEM((3072, 256), BF16),
            pltpu.VMEM((1024, FEATURES), BF16),
            pltpu.VMEM((1024, FEATURES), BF16),
            pltpu.VMEM((GROUPS, CHANNEL, STATE), F32),
            pltpu.VMEM((GROUPS, CHANNEL, STATE), F32),
            pltpu.VMEM((GROUPS, CHANNEL, STATE), F32),
            pltpu.VMEM((GROUPS, CHANNEL, STATE), F32),
            pltpu.VMEM((2, 64, 64), BF16),
            pltpu.VMEM((256, 2 * WIDTH), BF16),
            pltpu.VMEM((2 * WIDTH, 256), BF16),
            pltpu.VMEM((ROWS, ROWS), BF16),
            pltpu.VMEM((2 * ROWS, ROWS), BF16),
            pltpu.VMEM((2 * ROWS, REACH), BF16),
            pltpu.VMEM((ROWS, 128), F32),
            pltpu.VMEM((ROWS, 2 * WIDTH), F32),
            pltpu.VMEM((ROWS, 2 * WIDTH), BF16),
            pltpu.VMEM((ROWS, 2 * WIDTH), BF16),
            pltpu.VMEM((PEERS, 8, 128), F32),
            pltpu.VMEM((PEERS, REACH, 128), BF16),
            pltpu.VMEM((ROWS, 1024), BF16),
            pltpu.VMEM((ROWS, 1024), BF16),
            dma((16,)), dma((14,)), dma((14,)), dma((30,)), dma((30,)), dma((30,)), dma((30,)),
            pltpu.SemaphoreType.REGULAR, dma((PEERS,)), dma((PEERS,)), dma((1,)), dma((1,)), dma((14,)), dma((14,)), dma((7,)), dma((7,)),
        ],
        compiler_params=pltpu.CompilerParams(collective_id=0, has_side_effects=True, vmem_limit_bytes=60000000),
    )(*(pltpu.with_memory_space_constraint(v, pltpu.HBM) for v in (
        tokens, norm_gain.reshape(1, 3072), state_in_weight, pool_in_weight, rate_real, rate_imag,
        log_step.reshape(1, 64), jnp.swapaxes(input_real, 1, 2), jnp.swapaxes(input_imag, 1, 2), output_real, output_imag, skip_gain.reshape(1, 1024),
        pool_weight, pool_gain.reshape(1, 1024), state_out_weight, pool_out_weight,
    )))


def solution(mesh):
    tile = P("sp", "tp")
    in_specs = (tile, P(), tile, tile, *(P() for _ in range(10)), tile, tile)
    return jax.shard_map(body, mesh=mesh, in_specs=in_specs, out_specs=tile, check_vma=False)
```

```python
import functools

import jax
import jax.numpy as jnp
from jax import lax
from jax.experimental import pallas as pl
from jax.experimental.pallas import tpu as pltpu
from jax.sharding import PartitionSpec as P

EPSILON = 1e-06
HIGHEST = lax.Precision.HIGHEST
MESH = pl.DeviceIdType.MESH
F32, BF16 = jnp.float32, jnp.bfloat16

ROWS = 256
STEPS, PARTS = 32, 8
FEATURES = 384
PEERS, HEADS_TP = 16, 8
GROUPS, STATE, CHANNEL = 8, 64, 16
WIDTH = GROUPS * STATE
REACH = 16


def iota(shape, dim):
    return lax.broadcasted_iota(jnp.int32, shape, dim)


def position_of(row):
    return STEPS * (row % PARTS) + row // PARTS


def dot(a, b, precision=None):
    return jnp.dot(a, b, preferred_element_type=F32, precision=precision)


def split(value):
    high = value.astype(BF16)
    return high, (value - high.astype(F32)).astype(BF16)


class Move:
    def __init__(self, sends, fills, device, send_sem, recv_sem):
        self.sends, self.fills, self.device, self.send_sem, self.recv_sem = sends, fills, device, send_sem, recv_sem

    def copy(self, ref):
        return pltpu.make_async_remote_copy(
            src_ref=ref, dst_ref=ref, send_sem=self.send_sem, recv_sem=self.recv_sem,
            device_id=self.device, device_id_type=MESH)

    def start(self):
        self.copy(self.sends).start()

    def arrive(self):
        self.copy(self.fills).wait_recv()

    def arrive_all(self, ref):
        self.copy(ref).wait_recv()

    def left_all(self, ref):
        self.copy(ref).wait_send()


class LineGather:
    def __init__(self, slot, sems, first, shared, y, c):
        d = 1 - 2 * c
        at = lambda k, core: slot(lax.rem(y + k + 4, 4) * 2 + core)
        to = lambda k, core: {"tp": lax.rem(y + k + 4, 4) * 2 + core}
        o = 1 - c
        places = [first, first + 1, first + 2, shared[0], shared[0], shared[0], shared[1]]
        mk = lambda s, f, dev, i: Move(s, f, dev, sems[0].at[0], sems[1].at[places[i]])
        self.ahead = mk(at(0, c), at(-d, c), to(d, c), 0)
        self.back = mk(at(0, c), at(d, c), to(-d, c), 1)
        self.onward = mk(at(-d, c), at(-2 * d, c), to(d, c), 2)
        self.own = mk(at(0, c), at(0, o), to(0, o), 3)
        self.cross_ahead = mk(at(-d, c), at(d, o), to(0, o), 4)
        self.cross_back = mk(at(d, c), at(-d, o), to(0, o), 5)
        self.cross_far = mk(at(-2 * d, c), at(2 * d, o), to(0, o), 6)
        self.all = [self.ahead, self.back, self.onward, self.own, self.cross_ahead, self.cross_back, self.cross_far]
        index = lambda k, core: lax.rem(y + k + 4, 4) * 2 + core
        self.index = dict(own=index(0, c), ahead=index(-d, c), back=index(d, c), onward=index(-2 * d, c),
                          p_own=index(0, o), p_ahead=index(d, o), p_back=index(-d, o), p_onward=index(2 * d, o))


class PlaneGather:
    def __init__(self, slot_a, slot_b, sems, nine, z, x):
        wrap = lambda k: lax.rem(k + 4, 4)
        at = lambda dz, dx: wrap(z + dz) * 4 + wrap(x + dx)
        self.count, self.nine = 2, nine

        def mk(slot, half, sent, filled, device, shared):
            place = half if shared else self.count
            self.count += not shared
            return Move(slot(at(*sent)), slot(at(*filled)), {"sp": at(*device)}, sems[0].at[half], sems[1].at[place])

        def ring(half, along, e, base, straight, shared):
            slot = (slot_a, slot_b)[half]
            v = (lambda k: (base, k)) if along == "x" else (lambda k: (k, base))
            w = (lambda k: (0, k)) if along == "x" else (lambda k: (k, 0))
            third = (v(0), v(2), w(2)) if straight else (v(-e), v(-2 * e), w(e))
            return [
                mk(slot, half, v(0), v(-e), w(e), shared[0]),
                mk(slot, half, v(0), v(e), w(-e), shared[1]),
                mk(slot, half, *third, shared[2]),
            ]

        first, second, last = (False,) * 3, (False, True, True), (True,) * 3
        self.a = ring(0, "x", 1, 0, True, first)
        self.b = ring(1, "z", -1, 0, True, first)
        heavy = {0: 1, -1: -1, 1: -1, 2: 1}
        self.za = {o: ring(0, "z", heavy[o], o, o == 2, last if o == 2 else second) for o in (0, -1, 1, 2)}
        self.xb = {o: ring(1, "x", -heavy[o], o, o == 2, last if o == 2 else second) for o in (0, -1, 1, 2)}

    def begin(self):
        for ring in (self.a, self.b):
            ring[0].start()
            ring[1].start()
        for ring in (self.a, self.b):
            ring[2].start()
        for ring in (self.za[0], self.xb[0]):
            ring[0].start()
            ring[1].start()

    def events(self):
        def across(move, ring, count):
            def event():
                move.arrive()
                for k in range(count):
                    ring[k].start()
            return event

        def onward(ring):
            def event():
                ring[0].arrive()
                ring[2].start()
            return event

        def rest():
            self.za[2][0].arrive_all(self.nine[0])
            self.xb[2][0].arrive_all(self.nine[1])

        return [
            across(self.a[0], self.za[-1], 2), across(self.b[0], self.xb[1], 2),
            across(self.a[1], self.za[1], 2), across(self.b[1], self.xb[-1], 2),
            across(self.a[2], self.za[2], 3), across(self.b[2], self.xb[2], 3),
            onward(self.za[0]), onward(self.xb[0]),
            onward(self.za[-1]), onward(self.xb[1]), onward(self.za[1]), onward(self.xb[-1]), rest,
        ]


def kernel(
    tokens, gain_all, state_in_w, pool_in_w, rate_real_all, rate_imag_all, log_step_all, input_real, input_imag,
    output_real, output_imag, skip_all, pool_weight, pool_gain_all, state_out_w, pool_out_w, out,
    gain, rate_real, rate_imag, log_step, skip_gain, pool_gain, own_tokens, tok, scaled, win, wst, wpo, in_re, in_im, out_re, out_im, mix_raw,
    drive, read, unsort, bands, tails, recip, push, high, low, ends, halo, sbuf, pbuf,
    local_sem, tok_send, tok_recv, win_send, win_recv, wout_send, wout_recv,
    ready, end_send, end_recv, halo_send, halo_recv, s_send, s_recv, p_send, p_recv,
):
    s, t = lax.axis_index("sp"), lax.axis_index("tp")
    z, x, y, c = s // 4, s % 4, t // 2, t % 2
    g0 = t * GROUPS

    def lanes(ref, index, width):
        return ref.at[:, pl.ds(pl.multiple_of(index * width, 128), width)]

    def rows(ref, start, count):
        return ref.at[pl.ds(pl.multiple_of(start, 16), count), :]

    loads = [
        (tokens, own_tokens),
        (state_in_w, win.at[pl.ds(pl.multiple_of(s * 192, 16), 192), 0:128]),
        (pool_in_w, win.at[pl.ds(pl.multiple_of(s * 192, 16), 192), 128:256]),
        (state_out_w, rows(wst, s * 64, 64)),
        (pool_out_w, rows(wpo, s * 64, 64)),
        (input_real.at[pl.ds(g0, GROUPS)], in_re),
        (input_imag.at[pl.ds(g0, GROUPS)], in_im),
        (output_real.at[pl.ds(g0, GROUPS)], out_re),
        (output_imag.at[pl.ds(g0, GROUPS)], out_im),
        (pool_weight.at[pl.ds(2 * t, 2)], mix_raw),
        (gain_all, gain),
        (rate_real_all.at[pl.ds(pl.multiple_of(g0, 8), GROUPS), :], rate_real),
        (rate_imag_all.at[pl.ds(pl.multiple_of(g0, 8), GROUPS), :], rate_imag),
        (log_step_all, log_step),
        (lanes(skip_all, t, 128), skip_gain),
        (lanes(pool_gain_all, t, 128), pool_gain),
    ]
    loads = [pltpu.make_async_copy(a, b, local_sem.at[k]) for k, (a, b) in enumerate(loads)]
    for load in loads:
        load.start()

    barrier = pltpu.get_barrier_semaphore()
    beside = [z * 4 + lax.rem(x + k, 4) for k in (1, 2, 3)]
    above = [lax.rem(z + k, 4) * 4 + x for k in (1, 2, 3)]
    for peer in (*beside, *above):
        pl.semaphore_signal(barrier, inc=1, device_id={"sp": peer}, device_id_type=MESH)
    for k in range(1, HEADS_TP):
        pl.semaphore_signal(barrier, inc=1, device_id={"tp": lax.rem(t + k, HEADS_TP)}, device_id_type=MESH)

    r0, r1 = iota((ROWS, ROWS), 0), iota((ROWS, ROWS), 1)
    loads[0].wait()
    sort = (position_of(r0) == r1).astype(BF16)
    lanes(tok, t, FEATURES)[...] = dot(sort, own_tokens[...]).astype(BF16)
    unsort[...] = (position_of(r1) == r0).astype(BF16)

    def halves(ref, width, sems):
        def of(k):
            return lambda p: ref.at[pl.ds(k * 128, 128), pl.ds(pl.multiple_of(p * width, 128), width)]
        return [LineGather(of(k), sems, 3 * k, (6, 7), y, c) for k in range(2)]

    tok_lines = halves(tok, FEATURES, (tok_send, tok_recv))
    w_in = PlaneGather(
        lambda q: rows(win, q * 192, 96), lambda q: rows(win, q * 192 + 96, 96), (win_send, win_recv),
        (win.at[0:864], win.at[0:864]), z, x)
    w_out = PlaneGather(
        lambda q: rows(wst, q * 64, 64), lambda q: rows(wpo, q * 64, 64), (wout_send, wout_recv),
        (wst.at[0:576], wpo.at[0:576]), z, x)
    for load in loads[1:3]:
        load.wait()

    pl.semaphore_wait(barrier, 6 + HEADS_TP - 1)
    for line in tok_lines:
        line.ahead.start()
        line.back.start()
    w_in.begin()
    for line in tok_lines:
        line.own.start()
    for peer in beside:
        pl.semaphore_signal(ready, inc=1, device_id={"sp": peer}, device_id_type=MESH)
    for load in loads[3:]:
        load.wait()

    wanted = iota((GROUPS, STATE), 0) + g0
    steps_log = jnp.sum(jnp.where(iota((GROUPS, 64), 1) == wanted, log_step[...], 0.0), axis=1, keepdims=True)
    step = jnp.exp(steps_log) / float(ROWS * PEERS)
    real = rate_real[...]
    imag = rate_imag[...]
    exponent, angle = real * step, imag * step
    magnitude = jnp.exp(exponent)
    cosine, sine, half_sine = jnp.cos(angle), jnp.sin(angle), jnp.sin(0.5 * angle)
    decay_real, decay_imag = magnitude * cosine, magnitude * sine
    less = exponent * (1.0 + exponent * 0.5 * (1.0 + exponent * (1.0 / 3.0) * (1.0 + exponent * 0.25)))
    less = less * cosine - 2.0 * half_sine * half_sine
    denominator = real * real + imag * imag
    factor_real = (less * real + decay_imag * imag) / denominator
    factor_imag = (decay_imag * real - less * imag) / denominator

    spread = (iota((STATE, WIDTH), 1) % STATE == iota((STATE, WIDTH), 0)).astype(F32)
    own_group = iota((GROUPS, WIDTH), 1) // STATE == iota((GROUPS, WIDTH), 0)

    def flat(value):
        return jnp.sum(jnp.where(own_group, dot(value, spread, HIGHEST), 0.0), axis=0, keepdims=True)

    lr, li = flat(decay_real), flat(decay_imag)
    fr, fi = flat(factor_real), flat(factor_imag)

    def times(ar, ai, br, bi):
        return ar * br - ai * bi, ar * bi + ai * br

    pr, pi = lr, li
    for _ in range(5):
        pr, pi = times(pr, pi, pr, pi)
    part_real, part_imag = pr, pi
    for _ in range(3):
        pr, pi = times(pr, pi, pr, pi)
    block_real, block_imag = pr, pi
    sub = iota((PARTS, WIDTH), 0)
    up_real, up_imag = jnp.ones((PARTS, WIDTH), F32), jnp.zeros((PARTS, WIDTH), F32)
    down_real, down_imag = up_real, up_imag
    wr, wi = jnp.ones((1, WIDTH), F32), jnp.zeros((1, WIDTH), F32)
    for k in range(1, PARTS):
        wr, wi = times(wr, wi, part_real, part_imag)
        up_real, up_imag = jnp.where(sub == k, wr, up_real), jnp.where(sub == k, wi, up_imag)
        down_real = jnp.where(sub == PARTS - 1 - k, wr, down_real)
        down_imag = jnp.where(sub == PARTS - 1 - k, wi, down_imag)

    own_read = iota((128, WIDTH), 0) // CHANNEL == iota((128, WIDTH), 1) // STATE
    for k, ref in enumerate((in_re, in_im)):
        wide = jnp.where(own_read, dot(ref[...].reshape(128, STATE), spread, HIGHEST), 0.0)
        top, rest = split(wide)
        drive[0:128, k * WIDTH : (k + 1) * WIDTH] = top
        drive[128:256, k * WIDTH : (k + 1) * WIDTH] = rest
    cr = jnp.where(own_read, dot(out_re[...].reshape(128, STATE), spread, HIGHEST), 0.0)
    ci = jnp.where(own_read, dot(out_im[...].reshape(128, STATE), spread, HIGHEST), 0.0)
    for k, part in enumerate((cr * fr - ci * fi, -(cr * fi + ci * fr))):
        top, rest = split(jnp.transpose(part))
        read[k * WIDTH : (k + 1) * WIDTH, 0:128] = top
        read[k * WIDTH : (k + 1) * WIDTH, 128:256] = rest

    window0 = jnp.where(c == 0, 2, 8)
    p0, p1 = position_of(r0), position_of(r1)
    for k in range(2):
        w = window0 * (k + 1)
        bands[k * ROWS : (k + 1) * ROWS, :] = ((p1 <= p0) & (p1 > p0 - w)).astype(BF16)
        h0, h1 = position_of(iota((ROWS, REACH), 0)), iota((ROWS, REACH), 1) - REACH
        tails[k * ROWS : (k + 1) * ROWS, :] = (h1 > h0 - w).astype(BF16)
    first_head = iota((ROWS, 128), 1) < 64
    here = position_of(iota((ROWS, 128), 0)) + s * ROWS + 1
    recip[...] = 1.0 / jnp.minimum(here, jnp.where(first_head, window0, 2 * window0)).astype(F32)
    last = (position_of(iota((REACH, ROWS), 1)) == iota((REACH, ROWS), 0) + (ROWS - REACH)).astype(BF16)

    pair = (iota((64, 128), 1) % 64 == iota((64, 128), 0)).astype(BF16)
    mixer = jnp.where(
        iota((128, 128), 0) // 64 == iota((128, 128), 1) // 64, dot(mix_raw[...].reshape(128, 64), pair), 0.0
    ).astype(BF16)

    def prepare(p, squares):
        ref = lanes(tok, p, FEATURES)
        f = ref[...].astype(F32)
        lanes(scaled, p, FEATURES)[...] = (f * gain[:, pl.ds(pl.multiple_of(p * FEATURES, 128), FEATURES)]).astype(BF16)
        f = f * f
        return squares + (f[:, 0:128] + f[:, 128:256] + f[:, 256:384])

    squares = prepare(t, jnp.zeros((ROWS, 128), F32))

    def relay(line):
        line.ahead.arrive()
        line.onward.start()
        line.cross_ahead.start()
        line.back.arrive()
        line.cross_back.start()

    def relay_far(line):
        line.onward.arrive()
        line.cross_far.start()

    events, later = w_in.events(), w_out.events()
    one, two = tok_lines
    index = one.index

    def run(which, first, last):
        for e in which[first:last]:
            e()

    run(events, 0, 4)
    relay(one)
    run(events, 4, 8)
    relay(two)
    run(events, 8, 12)
    w_out.begin()
    relay_far(one)
    for name in ("ahead", "back"):
        squares = prepare(index[name], squares)
    relay_far(two)
    squares = prepare(index["onward"], squares)
    one.own.arrive_all(tok.at[:, 0 : 3 * FEATURES])
    for name in ("p_own", "p_ahead", "p_back"):
        squares = prepare(index[name], squares)
    one.cross_far.arrive_all(tok.at[:, 0:FEATURES])
    squares = prepare(index["p_onward"], squares)
    inverse = lax.rsqrt(jnp.sum(squares, axis=1, keepdims=True) / 3072.0 + EPSILON)
    events[12]()

    entry = (dot(scaled[...], win[...]) * inverse).astype(BF16)
    state_in, pool_in = entry[:, 0:128], entry[:, 128:256]

    pl.semaphore_wait(ready, 3)
    halo[s] = dot(last, pool_in).astype(BF16)
    back = lax.rem(s + PEERS - 1, PEERS)
    halo_move = Move(halo.at[s], halo.at[back], {"sp": lax.rem(s + 1, PEERS)}, halo_send.at[0], halo_recv.at[0])
    halo_move.start()

    push[...] = dot(jnp.concatenate([state_in, state_in], axis=1), drive[...])
    lrb, lib = jnp.broadcast_to(lr, (PARTS, WIDTH)), jnp.broadcast_to(li, (PARTS, WIDTH))

    def advance(j, carry):
        sr, si = carry
        at = pl.ds(pl.multiple_of(j * PARTS, PARTS), PARTS)
        nr = lrb * sr - lib * si + push[at, 0:WIDTH]
        ni = lrb * si + lib * sr + push[at, WIDTH : 2 * WIDTH]
        return nr, ni

    zero = jnp.zeros((PARTS, WIDTH), F32)
    er, ei = lax.fori_loop(0, STEPS, advance, (zero, zero), unroll=8)
    br, bi = times(er, ei, down_real, down_imag)
    br, bi = jnp.sum(br, axis=0, keepdims=True), jnp.sum(bi, axis=0, keepdims=True)
    lines = lambda row: [row[:, 128 * k : 128 * (k + 1)] for k in range(WIDTH // 128)]
    ends[s] = jnp.concatenate(lines(br) + lines(bi), axis=0)
    moves = [
        Move(ends.at[s], ends.at[lax.rem(s - k + PEERS, PEERS)], {"sp": lax.rem(s + k, PEERS)}, end_send.at[0],
             end_recv.at[0])
        for k in range(1, PEERS)
    ]
    for m in moves:
        m.start()

    sums = dot(bands[...], pool_in)
    halo_move.arrive()
    before = halo[back]
    before = jnp.where(s > 0, before.astype(F32), 0.0).astype(BF16)
    sums = sums + dot(tails[...], before)
    pooled = jnp.where(first_head, sums[0:ROWS], sums[ROWS : 2 * ROWS]) * recip[...] - pool_in.astype(F32)
    top, rest = split(pooled)
    projected = dot(top, mixer) + dot(rest, mixer)
    pool_out = (projected * pool_gain[...]).astype(BF16)
    lanes(pbuf, t, 128)[...] = dot(unsort[...], pool_out).astype(BF16)
    pline = LineGather(lambda p: lanes(pbuf, p, 128), (p_send, p_recv), 0, (3, 3), y, c)
    pline.ahead.start()
    pline.back.start()
    pline.own.start()

    kr, ki = jnp.where(sub >= 1, pltpu.roll(er, 1, 0), 0.0), jnp.where(sub >= 1, pltpu.roll(ei, 1, 0), 0.0)
    gr, gi = part_real, part_imag
    for hop in (1, 2, 4):
        tr = jnp.where(sub >= hop, pltpu.roll(kr, hop, 0), 0.0)
        ti = jnp.where(sub >= hop, pltpu.roll(ki, hop, 0), 0.0)
        ar, ai = times(tr, ti, gr, gi)
        kr, ki = kr + ar, ki + ai
        gr, gi = times(gr, gi, gr, gi)

    run(later, 0, 6)
    relay(pline)
    moves[0].arrive_all(ends.at[0 : PEERS - 1])
    qr = jnp.concatenate(lines(block_real), axis=0)
    qi = jnp.concatenate(lines(block_imag), axis=0)
    hr, hi = jnp.zeros_like(qr), jnp.zeros_like(qi)
    for q in range(PEERS - 1):
        piece = ends[q]
        ar, ai = times(hr, hi, qr, qi)
        hr, hi = jnp.where(q < s, ar + piece[0:4], hr), jnp.where(q < s, ai + piece[4:8], hi)
    hr = jnp.concatenate([hr[k : k + 1] for k in range(4)], axis=1)
    hi = jnp.concatenate([hi[k : k + 1] for k in range(4)], axis=1)
    ar, ai = times(up_real, up_imag, hr, hi)

    def advance_pair(j, carry):
        one = advance(2 * j, carry)
        two = advance(2 * j + 1, one)
        at = pl.ds(pl.multiple_of(j * 2 * PARTS, 2 * PARTS), 2 * PARTS)
        for k in range(2):
            top, rest = split(jnp.concatenate([one[k], two[k]], axis=0))
            high[at, k * WIDTH : (k + 1) * WIDTH] = top
            low[at, k * WIDTH : (k + 1) * WIDTH] = rest
        return two

    lax.fori_loop(0, STEPS // 2, advance_pair, (kr + ar, ki + ai), unroll=4)
    both = dot(high[...], read[...])
    readout = both[:, 0:128] + both[:, 128:256] + dot(low[...], read[:, 0:128])
    readout = readout + skip_gain[...] * state_in.astype(F32)
    state_out = jax.nn.gelu(readout).astype(BF16)
    lanes(sbuf, t, 128)[...] = dot(unsort[...], state_out).astype(BF16)
    s_lines = halves(sbuf, 128, (s_send, s_recv))
    for line in s_lines:
        line.ahead.start()
        line.back.start()
    for line in s_lines:
        line.own.start()
    run(later, 6, 12)
    relay_far(pline)
    for line in s_lines:
        relay(line)
    pline.own.arrive_all(pbuf.at[:, 0:512])
    later[12]()
    total = dot(pbuf[...], wpo[...])
    for line in s_lines:
        relay_far(line)
    s_lines[0].own.arrive_all(sbuf.at[:, 0 : 3 * 128])
    s_lines[0].cross_far.arrive_all(sbuf.at[:, 0:128])
    out[...] = (total + dot(sbuf[...], wst[...])).astype(BF16)

    one.own.left_all(tok.at[:, 0 : 7 * FEATURES])
    for plane, refs in ((w_in, (win.at[0:1440], win.at[0:1440])), (w_out, (wst.at[0:960], wpo.at[0:960]))):
        plane.a[0].left_all(refs[0])
        plane.b[0].left_all(refs[1])
    moves[0].left_all(ends.at[0 : PEERS - 1])
    pline.own.left_all(pbuf.at[:, 0:896])
    s_lines[0].own.left_all(sbuf.at[:, 0:896])
    halo_move.left_all(halo.at[0])


def body(
    tokens, norm_gain, state_in_weight, pool_in_weight, rate_real, rate_imag, log_step, input_real, input_imag,
    output_real, output_imag, skip_gain, pool_weight, pool_gain, state_out_weight, pool_out_weight,
):
    vmem = pl.BlockSpec(memory_space=pltpu.VMEM)
    dma = pltpu.SemaphoreType.DMA
    return pl.pallas_call(
        kernel,
        out_shape=pltpu.VMEM((ROWS, FEATURES), BF16),
        in_specs=[pl.BlockSpec(memory_space=pltpu.HBM)] * 16,
        out_specs=vmem,
        scratch_shapes=[
            pltpu.VMEM((1, 3072), F32),
            pltpu.VMEM((GROUPS, STATE), F32),
            pltpu.VMEM((GROUPS, STATE), F32),
            pltpu.VMEM((1, 64), F32),
            pltpu.VMEM((1, 128), F32),
            pltpu.VMEM((1, 128), F32),
            pltpu.VMEM((ROWS, FEATURES), BF16),
            pltpu.VMEM((ROWS, 3072), BF16),
            pltpu.VMEM((ROWS, 3072), BF16),
            pltpu.VMEM((3072, 256), BF16),
            pltpu.VMEM((1024, FEATURES), BF16),
            pltpu.VMEM((1024, FEATURES), BF16),
            pltpu.VMEM((GROUPS, CHANNEL, STATE), F32),
            pltpu.VMEM((GROUPS, CHANNEL, STATE), F32),
            pltpu.VMEM((GROUPS, CHANNEL, STATE), F32),
            pltpu.VMEM((GROUPS, CHANNEL, STATE), F32),
            pltpu.VMEM((2, 64, 64), BF16),
            pltpu.VMEM((256, 2 * WIDTH), BF16),
            pltpu.VMEM((2 * WIDTH, 256), BF16),
            pltpu.VMEM((ROWS, ROWS), BF16),
            pltpu.VMEM((2 * ROWS, ROWS), BF16),
            pltpu.VMEM((2 * ROWS, REACH), BF16),
            pltpu.VMEM((ROWS, 128), F32),
            pltpu.VMEM((ROWS, 2 * WIDTH), F32),
            pltpu.VMEM((ROWS, 2 * WIDTH), BF16),
            pltpu.VMEM((ROWS, 2 * WIDTH), BF16),
            pltpu.VMEM((PEERS, 8, 128), F32),
            pltpu.VMEM((PEERS, REACH, 128), BF16),
            pltpu.VMEM((ROWS, 1024), BF16),
            pltpu.VMEM((ROWS, 1024), BF16),
            dma((16,)), dma((1,)), dma((8,)), dma((2,)), dma((14,)), dma((2,)), dma((14,)),
            pltpu.SemaphoreType.REGULAR, dma((1,)), dma((1,)), dma((1,)), dma((1,)),
            dma((1,)), dma((8,)), dma((1,)), dma((4,)),
        ],
        compiler_params=pltpu.CompilerParams(collective_id=0, has_side_effects=True, vmem_limit_bytes=60000000),
    )(*(pltpu.with_memory_space_constraint(v, pltpu.HBM) for v in (
        tokens, norm_gain.reshape(1, 3072), state_in_weight, pool_in_weight, rate_real, rate_imag,
        log_step.reshape(1, 64), jnp.swapaxes(input_real, 1, 2), jnp.swapaxes(input_imag, 1, 2), output_real, output_imag, skip_gain.reshape(1, 1024),
        pool_weight, pool_gain.reshape(1, 1024), state_out_weight, pool_out_weight,
    )))


def solution(mesh):
    tile = P("sp", "tp")
    in_specs = (tile, P(), tile, tile, *(P() for _ in range(10)), tile, tile)
    return jax.shard_map(body, mesh=mesh, in_specs=in_specs, out_specs=tile, check_vma=False)
```

```python
import functools

import jax
import jax.numpy as jnp
from jax import lax
from jax.experimental import pallas as pl
from jax.experimental.pallas import tpu as pltpu
from jax.sharding import PartitionSpec as P

EPSILON = 1e-06
HIGHEST = lax.Precision.HIGHEST
MESH = pl.DeviceIdType.MESH
F32, BF16 = jnp.float32, jnp.bfloat16

ROWS = 256
STEPS, PARTS = 32, 8
FEATURES = 384
PEERS, HEADS_TP = 16, 8
GROUPS, STATE, CHANNEL = 8, 64, 16
WIDTH = GROUPS * STATE
REACH = 16


def iota(shape, dim):
    return lax.broadcasted_iota(jnp.int32, shape, dim)


def position_of(row):
    return STEPS * (row % PARTS) + row // PARTS


def dot(a, b, precision=None):
    return jnp.dot(a, b, preferred_element_type=F32, precision=precision)


def split(value):
    high = value.astype(BF16)
    return high, (value - high.astype(F32)).astype(BF16)


class Move:
    def __init__(self, sends, fills, device, send_sem, recv_sem):
        self.sends, self.fills, self.device, self.send_sem, self.recv_sem = sends, fills, device, send_sem, recv_sem

    def copy(self, ref):
        return pltpu.make_async_remote_copy(
            src_ref=ref, dst_ref=ref, send_sem=self.send_sem, recv_sem=self.recv_sem,
            device_id=self.device, device_id_type=MESH)

    def start(self):
        self.copy(self.sends).start()

    def arrive(self):
        self.copy(self.fills).wait_recv()

    def arrive_all(self, ref):
        self.copy(ref).wait_recv()

    def left_all(self, ref):
        self.copy(ref).wait_send()


class LineGather:
    def __init__(self, slot, sems, first, shared, y, c, across):
        d = 1 - 2 * c
        at = lambda k, core: slot(lax.rem(y + k + 4, 4) * 2 + core)
        to = lambda k, core: {"tp": lax.rem(y + k + 4, 4) * 2 + core}
        o = 1 - c
        places = [first, first + 1, first + 2, shared[0], shared[0], shared[0], shared[1]]
        mk = lambda s, f, dev, i: Move(s, f, dev, sems[0].at[0], sems[1].at[places[i]])
        self.ahead = mk(at(0, c), at(-d, c), to(d, c), 0)
        self.back = mk(at(0, c), at(d, c), to(-d, c), 1)
        self.onward = mk(at(-d, c), at(-2 * d, c), to(d, c), 2)
        self.own = mk(at(0, c), at(0, o), to(0, o), 3)
        self.cross_ahead = mk(at(-d, c), at(d, o), to(0, o), 4)
        self.cross_back = mk(at(d, c), at(-d, o), to(0, o), 5)
        self.across = across
        self.cross_far = mk(at(-d, c) if across else at(-2 * d, c), at(2 * d, o), to(d if across else 0, o), 6)
        self.all = [self.ahead, self.back, self.onward, self.own, self.cross_ahead, self.cross_back, self.cross_far]
        index = lambda k, core: lax.rem(y + k + 4, 4) * 2 + core
        self.index = dict(own=index(0, c), ahead=index(-d, c), back=index(d, c), onward=index(-2 * d, c),
                          p_own=index(0, o), p_ahead=index(d, o), p_back=index(-d, o), p_onward=index(2 * d, o))


class PlaneGather:
    def __init__(self, slot_a, slot_b, sems, nine, z, x):
        wrap = lambda k: lax.rem(k + 4, 4)
        at = lambda dz, dx: wrap(z + dz) * 4 + wrap(x + dx)
        self.count, self.nine = 2, nine

        def mk(slot, half, sent, filled, device, shared):
            place = half if shared else self.count
            self.count += not shared
            return Move(slot(at(*sent)), slot(at(*filled)), {"sp": at(*device)}, sems[0].at[half], sems[1].at[place])

        def ring(half, along, e, base, straight, shared):
            slot = (slot_a, slot_b)[half]
            v = (lambda k: (base, k)) if along == "x" else (lambda k: (k, base))
            w = (lambda k: (0, k)) if along == "x" else (lambda k: (k, 0))
            third = (v(0), v(2), w(2)) if straight else (v(-e), v(-2 * e), w(e))
            return [
                mk(slot, half, v(0), v(-e), w(e), shared[0]),
                mk(slot, half, v(0), v(e), w(-e), shared[1]),
                mk(slot, half, *third, shared[2]),
            ]

        first, second, last = (False,) * 3, (False, True, True), (True,) * 3
        self.a = ring(0, "x", 1, 0, True, first)
        self.b = ring(1, "z", -1, 0, True, first)
        heavy = {0: 1, -1: -1, 1: -1, 2: 1}
        self.za = {o: ring(0, "z", heavy[o], o, o == 2, last if o == 2 else second) for o in (0, -1, 1, 2)}
        self.xb = {o: ring(1, "x", -heavy[o], o, o == 2, last if o == 2 else second) for o in (0, -1, 1, 2)}

    def begin(self):
        for ring in (self.a, self.b):
            ring[0].start()
            ring[1].start()
        for ring in (self.a, self.b):
            ring[2].start()
        for ring in (self.za[0], self.xb[0]):
            ring[0].start()
            ring[1].start()

    def events(self):
        def across(move, ring, count):
            def event():
                move.arrive()
                for k in range(count):
                    ring[k].start()
            return event

        def onward(ring):
            def event():
                ring[0].arrive()
                ring[2].start()
            return event

        def rest():
            self.za[2][0].arrive_all(self.nine[0])
            self.xb[2][0].arrive_all(self.nine[1])

        return [
            across(self.a[0], self.za[-1], 2), across(self.b[0], self.xb[1], 2),
            across(self.a[1], self.za[1], 2), across(self.b[1], self.xb[-1], 2),
            across(self.a[2], self.za[2], 3), across(self.b[2], self.xb[2], 3),
            onward(self.za[0]), onward(self.xb[0]),
            onward(self.za[-1]), onward(self.xb[1]), onward(self.za[1]), onward(self.xb[-1]), rest,
        ]


def kernel(
    tokens, gain_all, state_in_w, pool_in_w, rate_real_all, rate_imag_all, log_step_all, input_real, input_imag,
    output_real, output_imag, skip_all, pool_weight, pool_gain_all, state_out_w, pool_out_w, out,
    gain, rate_real, rate_imag, log_step, skip_gain, pool_gain, own_tokens, tok, scaled, win, wst, wpo, in_re, in_im, out_re, out_im, mix_raw,
    drive, read, unsort, bands, tails, recip, push, high, low, ends, halo, sbuf, pbuf,
    local_sem, tok_send, tok_recv, win_send, win_recv, wout_send, wout_recv,
    ready, end_send, end_recv, halo_send, halo_recv, s_send, s_recv, p_send, p_recv,
):
    s, t = lax.axis_index("sp"), lax.axis_index("tp")
    z, x, y, c = s // 4, s % 4, t // 2, t % 2
    g0 = t * GROUPS

    def lanes(ref, index, width):
        return ref.at[:, pl.ds(pl.multiple_of(index * width, 128), width)]

    def rows(ref, start, count):
        return ref.at[pl.ds(pl.multiple_of(start, 16), count), :]

    loads = [
        (tokens, own_tokens),
        (state_in_w, win.at[pl.ds(pl.multiple_of(s * 192, 16), 192), 0:128]),
        (pool_in_w, win.at[pl.ds(pl.multiple_of(s * 192, 16), 192), 128:256]),
        (state_out_w, rows(wst, s * 64, 64)),
        (pool_out_w, rows(wpo, s * 64, 64)),
        (input_real.at[pl.ds(g0, GROUPS)], in_re),
        (input_imag.at[pl.ds(g0, GROUPS)], in_im),
        (output_real.at[pl.ds(g0, GROUPS)], out_re),
        (output_imag.at[pl.ds(g0, GROUPS)], out_im),
        (pool_weight.at[pl.ds(2 * t, 2)], mix_raw),
        (gain_all, gain),
        (rate_real_all.at[pl.ds(pl.multiple_of(g0, 8), GROUPS), :], rate_real),
        (rate_imag_all.at[pl.ds(pl.multiple_of(g0, 8), GROUPS), :], rate_imag),
        (log_step_all, log_step),
        (lanes(skip_all, t, 128), skip_gain),
        (lanes(pool_gain_all, t, 128), pool_gain),
    ]
    loads = [pltpu.make_async_copy(a, b, local_sem.at[k]) for k, (a, b) in enumerate(loads)]
    for load in loads:
        load.start()

    barrier = pltpu.get_barrier_semaphore()
    beside = [z * 4 + lax.rem(x + k, 4) for k in (1, 2, 3)]
    above = [lax.rem(z + k, 4) * 4 + x for k in (1, 2, 3)]
    for peer in (*beside, *above):
        pl.semaphore_signal(barrier, inc=1, device_id={"sp": peer}, device_id_type=MESH)
    for k in range(1, HEADS_TP):
        pl.semaphore_signal(barrier, inc=1, device_id={"tp": lax.rem(t + k, HEADS_TP)}, device_id_type=MESH)

    r0, r1 = iota((ROWS, ROWS), 0), iota((ROWS, ROWS), 1)
    loads[0].wait()
    sort = (position_of(r0) == r1).astype(BF16)
    lanes(tok, t, FEATURES)[...] = dot(sort, own_tokens[...]).astype(BF16)
    unsort[...] = (position_of(r1) == r0).astype(BF16)

    def halves(ref, width, sems, across):
        def of(k):
            return lambda p: ref.at[pl.ds(k * 128, 128), pl.ds(pl.multiple_of(p * width, 128), width)]
        return [LineGather(of(k), sems, 3 * k, (6, 7), y, c, across) for k in range(2)]

    tok_lines = halves(tok, FEATURES, (tok_send, tok_recv), False)
    w_in = PlaneGather(
        lambda q: rows(win, q * 192, 96), lambda q: rows(win, q * 192 + 96, 96), (win_send, win_recv),
        (win.at[0:864], win.at[0:864]), z, x)
    w_out = PlaneGather(
        lambda q: rows(wst, q * 64, 64), lambda q: rows(wpo, q * 64, 64), (wout_send, wout_recv),
        (wst.at[0:576], wpo.at[0:576]), z, x)
    for load in loads[1:3]:
        load.wait()

    pl.semaphore_wait(barrier, 6 + HEADS_TP - 1)
    for line in tok_lines:
        line.ahead.start()
        line.back.start()
    w_in.begin()
    for line in tok_lines:
        line.own.start()
    for peer in beside:
        pl.semaphore_signal(ready, inc=1, device_id={"sp": peer}, device_id_type=MESH)
    for load in loads[3:]:
        load.wait()

    wanted = iota((GROUPS, STATE), 0) + g0
    steps_log = jnp.sum(jnp.where(iota((GROUPS, 64), 1) == wanted, log_step[...], 0.0), axis=1, keepdims=True)
    step = jnp.exp(steps_log) / float(ROWS * PEERS)
    real = rate_real[...]
    imag = rate_imag[...]
    exponent, angle = real * step, imag * step
    magnitude = jnp.exp(exponent)
    cosine, sine, half_sine = jnp.cos(angle), jnp.sin(angle), jnp.sin(0.5 * angle)
    decay_real, decay_imag = magnitude * cosine, magnitude * sine
    less = exponent * (1.0 + exponent * 0.5 * (1.0 + exponent * (1.0 / 3.0) * (1.0 + exponent * 0.25)))
    less = less * cosine - 2.0 * half_sine * half_sine
    denominator = real * real + imag * imag
    factor_real = (less * real + decay_imag * imag) / denominator
    factor_imag = (decay_imag * real - less * imag) / denominator

    spread = (iota((STATE, WIDTH), 1) % STATE == iota((STATE, WIDTH), 0)).astype(F32)
    own_group = iota((GROUPS, WIDTH), 1) // STATE == iota((GROUPS, WIDTH), 0)

    def flat(value):
        return jnp.sum(jnp.where(own_group, dot(value, spread, HIGHEST), 0.0), axis=0, keepdims=True)

    lr, li = flat(decay_real), flat(decay_imag)
    fr, fi = flat(factor_real), flat(factor_imag)

    def times(ar, ai, br, bi):
        return ar * br - ai * bi, ar * bi + ai * br

    pr, pi = lr, li
    for _ in range(5):
        pr, pi = times(pr, pi, pr, pi)
    part_real, part_imag = pr, pi
    for _ in range(3):
        pr, pi = times(pr, pi, pr, pi)
    block_real, block_imag = pr, pi
    sub = iota((PARTS, WIDTH), 0)
    up_real, up_imag = jnp.ones((PARTS, WIDTH), F32), jnp.zeros((PARTS, WIDTH), F32)
    down_real, down_imag = up_real, up_imag
    wr, wi = jnp.ones((1, WIDTH), F32), jnp.zeros((1, WIDTH), F32)
    for k in range(1, PARTS):
        wr, wi = times(wr, wi, part_real, part_imag)
        up_real, up_imag = jnp.where(sub == k, wr, up_real), jnp.where(sub == k, wi, up_imag)
        down_real = jnp.where(sub == PARTS - 1 - k, wr, down_real)
        down_imag = jnp.where(sub == PARTS - 1 - k, wi, down_imag)

    own_read = iota((128, WIDTH), 0) // CHANNEL == iota((128, WIDTH), 1) // STATE
    for k, ref in enumerate((in_re, in_im)):
        wide = jnp.where(own_read, dot(ref[...].reshape(128, STATE), spread, HIGHEST), 0.0)
        top, rest = split(wide)
        drive[0:128, k * WIDTH : (k + 1) * WIDTH] = top
        drive[128:256, k * WIDTH : (k + 1) * WIDTH] = rest
    cr = jnp.where(own_read, dot(out_re[...].reshape(128, STATE), spread, HIGHEST), 0.0)
    ci = jnp.where(own_read, dot(out_im[...].reshape(128, STATE), spread, HIGHEST), 0.0)
    for k, part in enumerate((cr * fr - ci * fi, -(cr * fi + ci * fr))):
        top, rest = split(jnp.transpose(part))
        read[k * WIDTH : (k + 1) * WIDTH, 0:128] = top
        read[k * WIDTH : (k + 1) * WIDTH, 128:256] = rest

    window0 = jnp.where(c == 0, 2, 8)
    p0, p1 = position_of(r0), position_of(r1)
    for k in range(2):
        w = window0 * (k + 1)
        bands[k * ROWS : (k + 1) * ROWS, :] = ((p1 <= p0) & (p1 > p0 - w)).astype(BF16)
        h0, h1 = position_of(iota((ROWS, REACH), 0)), iota((ROWS, REACH), 1) - REACH
        tails[k * ROWS : (k + 1) * ROWS, :] = (h1 > h0 - w).astype(BF16)
    first_head = iota((ROWS, 128), 1) < 64
    here = position_of(iota((ROWS, 128), 0)) + s * ROWS + 1
    recip[...] = 1.0 / jnp.minimum(here, jnp.where(first_head, window0, 2 * window0)).astype(F32)
    last = (position_of(iota((REACH, ROWS), 1)) == iota((REACH, ROWS), 0) + (ROWS - REACH)).astype(BF16)

    pair = (iota((64, 128), 1) % 64 == iota((64, 128), 0)).astype(BF16)
    mixer = jnp.where(
        iota((128, 128), 0) // 64 == iota((128, 128), 1) // 64, dot(mix_raw[...].reshape(128, 64), pair), 0.0
    ).astype(BF16)

    def prepare(p, squares):
        ref = lanes(tok, p, FEATURES)
        f = ref[...].astype(F32)
        lanes(scaled, p, FEATURES)[...] = (f * gain[:, pl.ds(pl.multiple_of(p * FEATURES, 128), FEATURES)]).astype(BF16)
        f = f * f
        return squares + (f[:, 0:128] + f[:, 128:256] + f[:, 256:384])

    squares = prepare(t, jnp.zeros((ROWS, 128), F32))

    def relay(line):
        line.ahead.arrive()
        line.onward.start()
        if line.across:
            line.cross_far.start()
        line.cross_ahead.start()
        line.back.arrive()
        line.cross_back.start()

    def relay_far(line):
        line.onward.arrive()
        if not line.across:
            line.cross_far.start()

    events, later = w_in.events(), w_out.events()
    one, two = tok_lines
    index = one.index

    def run(which, first, last):
        for e in which[first:last]:
            e()

    run(events, 0, 4)
    relay(one)
    run(events, 4, 8)
    relay(two)
    run(events, 8, 12)
    w_out.begin()
    relay_far(one)
    for name in ("ahead", "back"):
        squares = prepare(index[name], squares)
    relay_far(two)
    squares = prepare(index["onward"], squares)
    one.own.arrive_all(tok.at[:, 0 : 3 * FEATURES])
    for name in ("p_own", "p_ahead", "p_back"):
        squares = prepare(index[name], squares)
    one.cross_far.arrive_all(tok.at[:, 0:FEATURES])
    squares = prepare(index["p_onward"], squares)
    inverse = lax.rsqrt(jnp.sum(squares, axis=1, keepdims=True) / 3072.0 + EPSILON)
    events[12]()

    entry = (dot(scaled[...], win[...]) * inverse).astype(BF16)
    state_in, pool_in = entry[:, 0:128], entry[:, 128:256]

    pl.semaphore_wait(ready, 3)
    halo[s] = dot(last, pool_in).astype(BF16)
    back = lax.rem(s + PEERS - 1, PEERS)
    halo_move = Move(halo.at[s], halo.at[back], {"sp": lax.rem(s + 1, PEERS)}, halo_send.at[0], halo_recv.at[0])
    halo_move.start()

    push[...] = dot(jnp.concatenate([state_in, state_in], axis=1), drive[...])
    lrb, lib = jnp.broadcast_to(lr, (PARTS, WIDTH)), jnp.broadcast_to(li, (PARTS, WIDTH))

    def advance(j, carry):
        sr, si = carry
        at = pl.ds(pl.multiple_of(j * PARTS, PARTS), PARTS)
        nr = lrb * sr - lib * si + push[at, 0:WIDTH]
        ni = lrb * si + lib * sr + push[at, WIDTH : 2 * WIDTH]
        return nr, ni

    zero = jnp.zeros((PARTS, WIDTH), F32)
    er, ei = lax.fori_loop(0, STEPS, advance, (zero, zero), unroll=8)
    br, bi = times(er, ei, down_real, down_imag)
    br, bi = jnp.sum(br, axis=0, keepdims=True), jnp.sum(bi, axis=0, keepdims=True)
    lines = lambda row: [row[:, 128 * k : 128 * (k + 1)] for k in range(WIDTH // 128)]
    ends[s] = jnp.concatenate(lines(br) + lines(bi), axis=0)
    moves = [
        Move(ends.at[s], ends.at[lax.rem(s - k + PEERS, PEERS)], {"sp": lax.rem(s + k, PEERS)}, end_send.at[0],
             end_recv.at[0])
        for k in range(1, PEERS)
    ]
    for m in moves:
        m.start()

    sums = dot(bands[...], pool_in)
    halo_move.arrive()
    before = halo[back]
    before = jnp.where(s > 0, before.astype(F32), 0.0).astype(BF16)
    sums = sums + dot(tails[...], before)
    pooled = jnp.where(first_head, sums[0:ROWS], sums[ROWS : 2 * ROWS]) * recip[...] - pool_in.astype(F32)
    top, rest = split(pooled)
    projected = dot(top, mixer) + dot(rest, mixer)
    pool_out = (projected * pool_gain[...]).astype(BF16)
    lanes(pbuf, t, 128)[...] = dot(unsort[...], pool_out).astype(BF16)
    pline = LineGather(lambda p: lanes(pbuf, p, 128), (p_send, p_recv), 0, (3, 3), y, c, True)
    pline.ahead.start()
    pline.back.start()
    pline.own.start()

    kr, ki = jnp.where(sub >= 1, pltpu.roll(er, 1, 0), 0.0), jnp.where(sub >= 1, pltpu.roll(ei, 1, 0), 0.0)
    gr, gi = part_real, part_imag
    for hop in (1, 2, 4):
        tr = jnp.where(sub >= hop, pltpu.roll(kr, hop, 0), 0.0)
        ti = jnp.where(sub >= hop, pltpu.roll(ki, hop, 0), 0.0)
        ar, ai = times(tr, ti, gr, gi)
        kr, ki = kr + ar, ki + ai
        gr, gi = times(gr, gi, gr, gi)

    run(later, 0, 6)
    moves[0].arrive_all(ends.at[0 : PEERS - 1])
    qr = jnp.concatenate(lines(block_real), axis=0)
    qi = jnp.concatenate(lines(block_imag), axis=0)
    hr, hi = jnp.zeros_like(qr), jnp.zeros_like(qi)
    for q in range(PEERS - 1):
        piece = ends[q]
        ar, ai = times(hr, hi, qr, qi)
        hr, hi = jnp.where(q < s, ar + piece[0:4], hr), jnp.where(q < s, ai + piece[4:8], hi)
    hr = jnp.concatenate([hr[k : k + 1] for k in range(4)], axis=1)
    hi = jnp.concatenate([hi[k : k + 1] for k in range(4)], axis=1)
    ar, ai = times(up_real, up_imag, hr, hi)

    def advance_pair(j, carry):
        one = advance(2 * j, carry)
        two = advance(2 * j + 1, one)
        at = pl.ds(pl.multiple_of(j * 2 * PARTS, 2 * PARTS), 2 * PARTS)
        for k in range(2):
            top, rest = split(jnp.concatenate([one[k], two[k]], axis=0))
            high[at, k * WIDTH : (k + 1) * WIDTH] = top
            low[at, k * WIDTH : (k + 1) * WIDTH] = rest
        return two

    lax.fori_loop(0, STEPS // 2, advance_pair, (kr + ar, ki + ai), unroll=4)
    both = dot(high[...], read[...])
    readout = both[:, 0:128] + both[:, 128:256] + dot(low[...], read[:, 0:128])
    readout = readout + skip_gain[...] * state_in.astype(F32)
    state_out = jax.nn.gelu(readout).astype(BF16)
    lanes(sbuf, t, 128)[...] = dot(unsort[...], state_out).astype(BF16)
    s_lines = halves(sbuf, 128, (s_send, s_recv), True)
    for line in s_lines:
        line.ahead.start()
        line.back.start()
    for line in s_lines:
        line.own.start()
    relay(pline)
    for line in s_lines:
        relay(line)
    run(later, 6, 12)
    relay_far(pline)
    pline.own.arrive_all(pbuf.at[:, 0:512])
    later[12]()
    total = dot(pbuf[...], wpo[...])
    for line in s_lines:
        relay_far(line)
    s_lines[0].own.arrive_all(sbuf.at[:, 0 : 3 * 128])
    s_lines[0].cross_far.arrive_all(sbuf.at[:, 0:128])
    out[...] = (total + dot(sbuf[...], wst[...])).astype(BF16)

    one.own.left_all(tok.at[:, 0 : 7 * FEATURES])
    for plane, refs in ((w_in, (win.at[0:1440], win.at[0:1440])), (w_out, (wst.at[0:960], wpo.at[0:960]))):
        plane.a[0].left_all(refs[0])
        plane.b[0].left_all(refs[1])
    moves[0].left_all(ends.at[0 : PEERS - 1])
    pline.own.left_all(pbuf.at[:, 0:896])
    s_lines[0].own.left_all(sbuf.at[:, 0:896])
    halo_move.left_all(halo.at[0])


def body(
    tokens, norm_gain, state_in_weight, pool_in_weight, rate_real, rate_imag, log_step, input_real, input_imag,
    output_real, output_imag, skip_gain, pool_weight, pool_gain, state_out_weight, pool_out_weight,
):
    vmem = pl.BlockSpec(memory_space=pltpu.VMEM)
    dma = pltpu.SemaphoreType.DMA
    return pl.pallas_call(
        kernel,
        out_shape=pltpu.VMEM((ROWS, FEATURES), BF16),
        in_specs=[pl.BlockSpec(memory_space=pltpu.HBM)] * 16,
        out_specs=vmem,
        scratch_shapes=[
            pltpu.VMEM((1, 3072), F32),
            pltpu.VMEM((GROUPS, STATE), F32),
            pltpu.VMEM((GROUPS, STATE), F32),
            pltpu.VMEM((1, 64), F32),
            pltpu.VMEM((1, 128), F32),
            pltpu.VMEM((1, 128), F32),
            pltpu.VMEM((ROWS, FEATURES), BF16),
            pltpu.VMEM((ROWS, 3072), BF16),
            pltpu.VMEM((ROWS, 3072), BF16),
            pltpu.VMEM((3072, 256), BF16),
            pltpu.VMEM((1024, FEATURES), BF16),
            pltpu.VMEM((1024, FEATURES), BF16),
            pltpu.VMEM((GROUPS, CHANNEL, STATE), F32),
            pltpu.VMEM((GROUPS, CHANNEL, STATE), F32),
            pltpu.VMEM((GROUPS, CHANNEL, STATE), F32),
            pltpu.VMEM((GROUPS, CHANNEL, STATE), F32),
            pltpu.VMEM((2, 64, 64), BF16),
            pltpu.VMEM((256, 2 * WIDTH), BF16),
            pltpu.VMEM((2 * WIDTH, 256), BF16),
            pltpu.VMEM((ROWS, ROWS), BF16),
            pltpu.VMEM((2 * ROWS, ROWS), BF16),
            pltpu.VMEM((2 * ROWS, REACH), BF16),
            pltpu.VMEM((ROWS, 128), F32),
            pltpu.VMEM((ROWS, 2 * WIDTH), F32),
            pltpu.VMEM((ROWS, 2 * WIDTH), BF16),
            pltpu.VMEM((ROWS, 2 * WIDTH), BF16),
            pltpu.VMEM((PEERS, 8, 128), F32),
            pltpu.VMEM((PEERS, REACH, 128), BF16),
            pltpu.VMEM((ROWS, 1024), BF16),
            pltpu.VMEM((ROWS, 1024), BF16),
            dma((16,)), dma((1,)), dma((8,)), dma((2,)), dma((14,)), dma((2,)), dma((14,)),
            pltpu.SemaphoreType.REGULAR, dma((1,)), dma((1,)), dma((1,)), dma((1,)),
            dma((1,)), dma((8,)), dma((1,)), dma((4,)),
        ],
        compiler_params=pltpu.CompilerParams(collective_id=0, has_side_effects=True, vmem_limit_bytes=60000000),
    )(*(pltpu.with_memory_space_constraint(v, pltpu.HBM) for v in (
        tokens, norm_gain.reshape(1, 3072), state_in_weight, pool_in_weight, rate_real, rate_imag,
        log_step.reshape(1, 64), jnp.swapaxes(input_real, 1, 2), jnp.swapaxes(input_imag, 1, 2), output_real, output_imag, skip_gain.reshape(1, 1024),
        pool_weight, pool_gain.reshape(1, 1024), state_out_weight, pool_out_weight,
    )))


def solution(mesh):
    tile = P("sp", "tp")
    in_specs = (tile, P(), tile, tile, *(P() for _ in range(10)), tile, tile)
    return jax.shard_map(body, mesh=mesh, in_specs=in_specs, out_specs=tile, check_vma=False)
```

```python
import functools

import jax
import jax.numpy as jnp
from jax import lax
from jax.experimental import pallas as pl
from jax.experimental.pallas import tpu as pltpu
from jax.sharding import PartitionSpec as P

EPSILON = 1e-06
HIGHEST = lax.Precision.HIGHEST
MESH = pl.DeviceIdType.MESH
F32, BF16 = jnp.float32, jnp.bfloat16

ROWS = 256
STEPS, PARTS = 32, 8
FEATURES = 384
PEERS, HEADS_TP = 16, 8
GROUPS, STATE, CHANNEL = 8, 64, 16
WIDTH = GROUPS * STATE
REACH = 16


def iota(shape, dim):
    return lax.broadcasted_iota(jnp.int32, shape, dim)


def position_of(row):
    return STEPS * (row % PARTS) + row // PARTS


def dot(a, b, precision=None):
    return jnp.dot(a, b, preferred_element_type=F32, precision=precision)


def split(value):
    high = value.astype(BF16)
    return high, (value - high.astype(F32)).astype(BF16)


class Move:
    def __init__(self, sends, fills, device, send_sem, recv_sem):
        self.sends, self.fills, self.device, self.send_sem, self.recv_sem = sends, fills, device, send_sem, recv_sem

    def copy(self, ref):
        return pltpu.make_async_remote_copy(
            src_ref=ref, dst_ref=ref, send_sem=self.send_sem, recv_sem=self.recv_sem,
            device_id=self.device, device_id_type=MESH)

    def start(self):
        self.copy(self.sends).start()

    def arrive(self):
        self.copy(self.fills).wait_recv()

    def arrive_all(self, ref):
        self.copy(ref).wait_recv()

    def left_all(self, ref):
        self.copy(ref).wait_send()


class LineGather:
    def __init__(self, slot, sems, first, shared, y, c, across):
        d = 1 - 2 * c
        at = lambda k, core: slot(lax.rem(y + k + 4, 4) * 2 + core)
        to = lambda k, core: {"tp": lax.rem(y + k + 4, 4) * 2 + core}
        o = 1 - c
        places = [first, first + 1, first + 2, shared[0], shared[0], shared[0], shared[1]]
        mk = lambda s, f, dev, i: Move(s, f, dev, sems[0].at[0], sems[1].at[places[i]])
        self.ahead = mk(at(0, c), at(-d, c), to(d, c), 0)
        self.back = mk(at(0, c), at(d, c), to(-d, c), 1)
        self.onward = mk(at(-d, c), at(-2 * d, c), to(d, c), 2)
        self.own = mk(at(0, c), at(0, o), to(0, o), 3)
        self.cross_ahead = mk(at(-d, c), at(d, o), to(0, o), 4)
        self.cross_back = mk(at(d, c), at(-d, o), to(0, o), 5)
        self.across = across
        self.cross_far = mk(at(-d, c) if across else at(-2 * d, c), at(2 * d, o), to(d if across else 0, o), 6)
        self.all = [self.ahead, self.back, self.onward, self.own, self.cross_ahead, self.cross_back, self.cross_far]
        index = lambda k, core: lax.rem(y + k + 4, 4) * 2 + core
        self.index = dict(own=index(0, c), ahead=index(-d, c), back=index(d, c), onward=index(-2 * d, c),
                          p_own=index(0, o), p_ahead=index(d, o), p_back=index(-d, o), p_onward=index(2 * d, o))


class PlaneGather:
    def __init__(self, slot_a, slot_b, sems, sized, z, x):
        wrap = lambda k: lax.rem(k + 4, 4)
        at = lambda dz, dx: wrap(z + dz) * 4 + wrap(x + dx)
        self.count, self.sized, self.groups, self.places = 0, sized, {}, {}

        def mk(half, sent, filled, device, key=None):
            slot = (slot_a, slot_b)[half]
            place = self.places.get(key, self.count)
            if place == self.count:
                self.count += 1
            move = Move(slot(at(*sent)), slot(at(*filled)), {"sp": at(*device)}, sems[0].at[half], sems[1].at[place])
            if key is not None:
                self.places[key] = place
                self.groups.setdefault(key, []).append(move)
            return move

        def ring(half, along, e, base):
            v = (lambda k: (base, k)) if along == "x" else (lambda k: (k, base))
            w = (lambda k: (0, k)) if along == "x" else (lambda k: (k, 0))
            key = lambda k: (half, base if along == "x" else k)
            return [
                mk(half, v(0), v(-e), w(e)),
                mk(half, v(0), v(e), w(-e), key(e)),
                mk(half, v(-e), v(-2 * e), w(e), key(2)),
            ]

        self.a = [mk(0, (0, 0), (0, -k), (0, k)) for k in (1, -1, 2)]
        self.b = [mk(1, (0, 0), (-k, 0), (k, 0)) for k in (-1, 1, 2)]
        heavy = {0: 1, -1: -1, 1: -1, 2: 1}
        self.za = {o: ring(0, "z", heavy[o], o) for o in (0, -1, 1, 2)}
        self.xb = {o: ring(1, "x", -heavy[o], o) for o in (0, -1, 1, 2)}

    def ready(self, dz):
        for half in (0, 1):
            group = self.groups.get((half, dz), [])
            if group:
                group[0].arrive_all(self.sized(half, len(group)))

    def begin(self):
        for ring in (self.a, self.b):
            ring[0].start()
            ring[1].start()
        for ring in (self.a, self.b):
            ring[2].start()
        for ring in (self.za[0], self.xb[0]):
            ring[0].start()
            ring[1].start()

    def events(self):
        def across(move, ring, count):
            def event():
                move.arrive()
                for k in range(count):
                    ring[k].start()
            return event

        def onward(ring):
            def event():
                ring[0].arrive()
                ring[2].start()
            return event

        return [
            across(self.a[0], self.za[-1], 2), across(self.b[0], self.xb[1], 2),
            across(self.a[1], self.za[1], 2), across(self.b[1], self.xb[-1], 2),
            across(self.a[2], self.za[2], 2), across(self.b[2], self.xb[2], 2),
            onward(self.za[0]), onward(self.xb[0]),
            onward(self.za[-1]), onward(self.xb[1]), onward(self.za[1]), onward(self.xb[-1]),
            onward(self.za[2]), onward(self.xb[2]),
        ]


def kernel(
    tokens, gain_all, state_in_w, pool_in_w, rate_real_all, rate_imag_all, log_step_all, input_real, input_imag,
    output_real, output_imag, skip_all, pool_weight, pool_gain_all, state_out_w, pool_out_w, out,
    gain, rate_real, rate_imag, log_step, skip_gain, pool_gain, own_tokens, tok, scaled, win, wst, wpo, in_re, in_im, out_re, out_im, mix_raw,
    drive, read, unsort, bands, tails, recip, push, high, low, ends, halo, sbuf, pbuf,
    local_sem, tok_send, tok_recv, win_send, win_recv, wout_send, wout_recv,
    ready, end_send, end_recv, halo_send, halo_recv, s_send, s_recv, p_send, p_recv,
):
    s, t = lax.axis_index("sp"), lax.axis_index("tp")
    z, x, y, c = s // 4, s % 4, t // 2, t % 2
    g0 = t * GROUPS

    def lanes(ref, index, width):
        return ref.at[:, pl.ds(pl.multiple_of(index * width, 128), width)]

    def rows(ref, start, count):
        return ref.at[pl.ds(pl.multiple_of(start, 16), count), :]

    loads = [
        (tokens, own_tokens),
        (state_in_w, win.at[pl.ds(pl.multiple_of(s * 192, 16), 192), 0:128]),
        (pool_in_w, win.at[pl.ds(pl.multiple_of(s * 192, 16), 192), 128:256]),
        (state_out_w, rows(wst, s * 64, 64)),
        (pool_out_w, rows(wpo, s * 64, 64)),
        (input_real.at[pl.ds(g0, GROUPS)], in_re),
        (input_imag.at[pl.ds(g0, GROUPS)], in_im),
        (output_real.at[pl.ds(g0, GROUPS)], out_re),
        (output_imag.at[pl.ds(g0, GROUPS)], out_im),
        (pool_weight.at[pl.ds(2 * t, 2)], mix_raw),
        (gain_all, gain),
        (rate_real_all.at[pl.ds(pl.multiple_of(g0, 8), GROUPS), :], rate_real),
        (rate_imag_all.at[pl.ds(pl.multiple_of(g0, 8), GROUPS), :], rate_imag),
        (log_step_all, log_step),
        (lanes(skip_all, t, 128), skip_gain),
        (lanes(pool_gain_all, t, 128), pool_gain),
    ]
    loads = [pltpu.make_async_copy(a, b, local_sem.at[k]) for k, (a, b) in enumerate(loads)]
    for load in loads:
        load.start()

    barrier = pltpu.get_barrier_semaphore()
    beside = [z * 4 + lax.rem(x + k, 4) for k in (1, 2, 3)]
    above = [lax.rem(z + k, 4) * 4 + x for k in (1, 2, 3)]
    for peer in (*beside, *above):
        pl.semaphore_signal(barrier, inc=1, device_id={"sp": peer}, device_id_type=MESH)
    for k in range(1, HEADS_TP):
        pl.semaphore_signal(barrier, inc=1, device_id={"tp": lax.rem(t + k, HEADS_TP)}, device_id_type=MESH)

    r0, r1 = iota((ROWS, ROWS), 0), iota((ROWS, ROWS), 1)
    loads[0].wait()
    sort = (position_of(r0) == r1).astype(BF16)
    lanes(tok, t, FEATURES)[...] = dot(sort, own_tokens[...]).astype(BF16)
    unsort[...] = (position_of(r1) == r0).astype(BF16)

    def halves(ref, width, sems, across):
        def of(k):
            return lambda p: ref.at[pl.ds(k * 128, 128), pl.ds(pl.multiple_of(p * width, 128), width)]
        return [LineGather(of(k), sems, 3 * k, (6, 7), y, c, across) for k in range(2)]

    tok_lines = halves(tok, FEATURES, (tok_send, tok_recv), False)
    w_in = PlaneGather(
        lambda q: rows(win, q * 192, 96), lambda q: rows(win, q * 192 + 96, 96), (win_send, win_recv),
        lambda half, n: win.at[0 : 96 * n], z, x)
    w_out = PlaneGather(
        lambda q: rows(wst, q * 64, 64), lambda q: rows(wpo, q * 64, 64), (wout_send, wout_recv),
        lambda half, n: (wst, wpo)[half].at[0 : 64 * n], z, x)
    for load in loads[1:3]:
        load.wait()

    pl.semaphore_wait(barrier, 6 + HEADS_TP - 1)
    for line in tok_lines:
        line.ahead.start()
        line.back.start()
    w_in.begin()
    for line in tok_lines:
        line.own.start()
    for peer in beside:
        pl.semaphore_signal(ready, inc=1, device_id={"sp": peer}, device_id_type=MESH)
    for load in loads[3:]:
        load.wait()

    wanted = iota((GROUPS, STATE), 0) + g0
    steps_log = jnp.sum(jnp.where(iota((GROUPS, 64), 1) == wanted, log_step[...], 0.0), axis=1, keepdims=True)
    step = jnp.exp(steps_log) / float(ROWS * PEERS)
    real = rate_real[...]
    imag = rate_imag[...]
    exponent, angle = real * step, imag * step
    magnitude = jnp.exp(exponent)
    cosine, sine, half_sine = jnp.cos(angle), jnp.sin(angle), jnp.sin(0.5 * angle)
    decay_real, decay_imag = magnitude * cosine, magnitude * sine
    less = exponent * (1.0 + exponent * 0.5 * (1.0 + exponent * (1.0 / 3.0) * (1.0 + exponent * 0.25)))
    less = less * cosine - 2.0 * half_sine * half_sine
    denominator = real * real + imag * imag
    factor_real = (less * real + decay_imag * imag) / denominator
    factor_imag = (decay_imag * real - less * imag) / denominator

    spread = (iota((STATE, WIDTH), 1) % STATE == iota((STATE, WIDTH), 0)).astype(F32)
    own_group = iota((GROUPS, WIDTH), 1) // STATE == iota((GROUPS, WIDTH), 0)

    def flat(value):
        return jnp.sum(jnp.where(own_group, dot(value, spread, HIGHEST), 0.0), axis=0, keepdims=True)

    lr, li = flat(decay_real), flat(decay_imag)
    fr, fi = flat(factor_real), flat(factor_imag)

    def times(ar, ai, br, bi):
        return ar * br - ai * bi, ar * bi + ai * br

    pr, pi = lr, li
    for _ in range(5):
        pr, pi = times(pr, pi, pr, pi)
    part_real, part_imag = pr, pi
    for _ in range(3):
        pr, pi = times(pr, pi, pr, pi)
    block_real, block_imag = pr, pi
    sub = iota((PARTS, WIDTH), 0)
    up_real, up_imag = jnp.ones((PARTS, WIDTH), F32), jnp.zeros((PARTS, WIDTH), F32)
    down_real, down_imag = up_real, up_imag
    wr, wi = jnp.ones((1, WIDTH), F32), jnp.zeros((1, WIDTH), F32)
    for k in range(1, PARTS):
        wr, wi = times(wr, wi, part_real, part_imag)
        up_real, up_imag = jnp.where(sub == k, wr, up_real), jnp.where(sub == k, wi, up_imag)
        down_real = jnp.where(sub == PARTS - 1 - k, wr, down_real)
        down_imag = jnp.where(sub == PARTS - 1 - k, wi, down_imag)

    own_read = iota((128, WIDTH), 0) // CHANNEL == iota((128, WIDTH), 1) // STATE
    for k, ref in enumerate((in_re, in_im)):
        wide = jnp.where(own_read, dot(ref[...].reshape(128, STATE), spread, HIGHEST), 0.0)
        top, rest = split(wide)
        drive[0:128, k * WIDTH : (k + 1) * WIDTH] = top
        drive[128:256, k * WIDTH : (k + 1) * WIDTH] = rest
    cr = jnp.where(own_read, dot(out_re[...].reshape(128, STATE), spread, HIGHEST), 0.0)
    ci = jnp.where(own_read, dot(out_im[...].reshape(128, STATE), spread, HIGHEST), 0.0)
    for k, part in enumerate((cr * fr - ci * fi, -(cr * fi + ci * fr))):
        top, rest = split(jnp.transpose(part))
        read[k * WIDTH : (k + 1) * WIDTH, 0:128] = top
        read[k * WIDTH : (k + 1) * WIDTH, 128:256] = rest

    window0 = jnp.where(c == 0, 2, 8)
    p0, p1 = position_of(r0), position_of(r1)
    for k in range(2):
        w = window0 * (k + 1)
        bands[k * ROWS : (k + 1) * ROWS, :] = ((p1 <= p0) & (p1 > p0 - w)).astype(BF16)
        h0, h1 = position_of(iota((ROWS, REACH), 0)), iota((ROWS, REACH), 1) - REACH
        tails[k * ROWS : (k + 1) * ROWS, :] = (h1 > h0 - w).astype(BF16)
    first_head = iota((ROWS, 128), 1) < 64
    here = position_of(iota((ROWS, 128), 0)) + s * ROWS + 1
    recip[...] = 1.0 / jnp.minimum(here, jnp.where(first_head, window0, 2 * window0)).astype(F32)
    last = (position_of(iota((REACH, ROWS), 1)) == iota((REACH, ROWS), 0) + (ROWS - REACH)).astype(BF16)

    pair = (iota((64, 128), 1) % 64 == iota((64, 128), 0)).astype(BF16)
    mixer = jnp.where(
        iota((128, 128), 0) // 64 == iota((128, 128), 1) // 64, dot(mix_raw[...].reshape(128, 64), pair), 0.0
    ).astype(BF16)

    def prepare(p, squares):
        ref = lanes(tok, p, FEATURES)
        f = ref[...].astype(F32)
        lanes(scaled, p, FEATURES)[...] = (f * gain[:, pl.ds(pl.multiple_of(p * FEATURES, 128), FEATURES)]).astype(BF16)
        f = f * f
        return squares + (f[:, 0:128] + f[:, 128:256] + f[:, 256:384])

    squares = prepare(t, jnp.zeros((ROWS, 128), F32))

    def relay(line):
        line.ahead.arrive()
        line.onward.start()
        if line.across:
            line.cross_far.start()
        line.cross_ahead.start()
        line.back.arrive()
        line.cross_back.start()

    def relay_far(line):
        line.onward.arrive()
        if not line.across:
            line.cross_far.start()

    events, later = w_in.events(), w_out.events()
    one, two = tok_lines
    index = one.index

    def run(which, first, last):
        for e in which[first:last]:
            e()

    run(events, 0, 4)
    relay(one)
    run(events, 4, 8)
    relay(two)
    run(events, 8, 14)
    w_out.begin()
    relay_far(one)
    for name in ("ahead", "back"):
        squares = prepare(index[name], squares)
    relay_far(two)
    squares = prepare(index["onward"], squares)
    one.own.arrive_all(tok.at[:, 0 : 3 * FEATURES])
    for name in ("p_own", "p_ahead", "p_back"):
        squares = prepare(index[name], squares)
    one.cross_far.arrive_all(tok.at[:, 0:FEATURES])
    squares = prepare(index["p_onward"], squares)
    inverse = lax.rsqrt(jnp.sum(squares, axis=1, keepdims=True) / 3072.0 + EPSILON)

    def row_part(ref, dz, width, axis):
        at = pl.ds(pl.multiple_of(lax.rem(z + dz + 4, 4) * width, 128), width)
        return ref[:, at] if axis else ref[at, :]

    product = jnp.zeros((ROWS, 256), F32)
    for dz in (0, 1, -1, 2):
        w_in.ready(dz)
        product = product + dot(row_part(scaled, dz, 768, 1), row_part(win, dz, 768, 0))
    entry = (product * inverse).astype(BF16)
    state_in, pool_in = entry[:, 0:128], entry[:, 128:256]

    pl.semaphore_wait(ready, 3)
    halo[s] = dot(last, pool_in).astype(BF16)
    back = lax.rem(s + PEERS - 1, PEERS)
    halo_move = Move(halo.at[s], halo.at[back], {"sp": lax.rem(s + 1, PEERS)}, halo_send.at[0], halo_recv.at[0])
    halo_move.start()

    push[...] = dot(jnp.concatenate([state_in, state_in], axis=1), drive[...])
    lrb, lib = jnp.broadcast_to(lr, (PARTS, WIDTH)), jnp.broadcast_to(li, (PARTS, WIDTH))

    def advance(j, carry):
        sr, si = carry
        at = pl.ds(pl.multiple_of(j * PARTS, PARTS), PARTS)
        nr = lrb * sr - lib * si + push[at, 0:WIDTH]
        ni = lrb * si + lib * sr + push[at, WIDTH : 2 * WIDTH]
        return nr, ni

    zero = jnp.zeros((PARTS, WIDTH), F32)
    er, ei = lax.fori_loop(0, STEPS, advance, (zero, zero), unroll=8)
    br, bi = times(er, ei, down_real, down_imag)
    br, bi = jnp.sum(br, axis=0, keepdims=True), jnp.sum(bi, axis=0, keepdims=True)
    lines = lambda row: [row[:, 128 * k : 128 * (k + 1)] for k in range(WIDTH // 128)]
    ends[s] = jnp.concatenate(lines(br) + lines(bi), axis=0)
    moves = [
        Move(ends.at[s], ends.at[lax.rem(s - k + PEERS, PEERS)], {"sp": lax.rem(s + k, PEERS)}, end_send.at[0],
             end_recv.at[0])
        for k in range(1, PEERS)
    ]
    for m in moves:
        m.start()

    sums = dot(bands[...], pool_in)
    halo_move.arrive()
    before = halo[back]
    before = jnp.where(s > 0, before.astype(F32), 0.0).astype(BF16)
    sums = sums + dot(tails[...], before)
    pooled = jnp.where(first_head, sums[0:ROWS], sums[ROWS : 2 * ROWS]) * recip[...] - pool_in.astype(F32)
    top, rest = split(pooled)
    projected = dot(top, mixer) + dot(rest, mixer)
    pool_out = (projected * pool_gain[...]).astype(BF16)
    lanes(pbuf, t, 128)[...] = dot(unsort[...], pool_out).astype(BF16)
    pline = LineGather(lambda p: lanes(pbuf, p, 128), (p_send, p_recv), 0, (3, 3), y, c, True)
    pline.ahead.start()
    pline.back.start()
    pline.own.start()

    kr, ki = jnp.where(sub >= 1, pltpu.roll(er, 1, 0), 0.0), jnp.where(sub >= 1, pltpu.roll(ei, 1, 0), 0.0)
    gr, gi = part_real, part_imag
    for hop in (1, 2, 4):
        tr = jnp.where(sub >= hop, pltpu.roll(kr, hop, 0), 0.0)
        ti = jnp.where(sub >= hop, pltpu.roll(ki, hop, 0), 0.0)
        ar, ai = times(tr, ti, gr, gi)
        kr, ki = kr + ar, ki + ai
        gr, gi = times(gr, gi, gr, gi)

    run(later, 0, 6)
    moves[0].arrive_all(ends.at[0 : PEERS - 1])
    qr = jnp.concatenate(lines(block_real), axis=0)
    qi = jnp.concatenate(lines(block_imag), axis=0)
    hr, hi = jnp.zeros_like(qr), jnp.zeros_like(qi)
    for q in range(PEERS - 1):
        piece = ends[q]
        ar, ai = times(hr, hi, qr, qi)
        hr, hi = jnp.where(q < s, ar + piece[0:4], hr), jnp.where(q < s, ai + piece[4:8], hi)
    hr = jnp.concatenate([hr[k : k + 1] for k in range(4)], axis=1)
    hi = jnp.concatenate([hi[k : k + 1] for k in range(4)], axis=1)
    ar, ai = times(up_real, up_imag, hr, hi)

    def advance_pair(j, carry):
        one = advance(2 * j, carry)
        two = advance(2 * j + 1, one)
        at = pl.ds(pl.multiple_of(j * 2 * PARTS, 2 * PARTS), 2 * PARTS)
        for k in range(2):
            top, rest = split(jnp.concatenate([one[k], two[k]], axis=0))
            high[at, k * WIDTH : (k + 1) * WIDTH] = top
            low[at, k * WIDTH : (k + 1) * WIDTH] = rest
        return two

    lax.fori_loop(0, STEPS // 2, advance_pair, (kr + ar, ki + ai), unroll=4)
    both = dot(high[...], read[...])
    readout = both[:, 0:128] + both[:, 128:256] + dot(low[...], read[:, 0:128])
    readout = readout + skip_gain[...] * state_in.astype(F32)
    state_out = jax.nn.gelu(readout).astype(BF16)
    lanes(sbuf, t, 128)[...] = dot(unsort[...], state_out).astype(BF16)
    s_lines = halves(sbuf, 128, (s_send, s_recv), True)
    for line in s_lines:
        line.ahead.start()
        line.back.start()
    for line in s_lines:
        line.own.start()
    relay(pline)
    for line in s_lines:
        relay(line)
    run(later, 6, 14)
    relay_far(pline)
    pline.own.arrive_all(pbuf.at[:, 0:512])
    total = jnp.zeros((ROWS, FEATURES), F32)
    for dz in (0, 1, -1):
        w_out.ready(dz)
        total = total + dot(row_part(pbuf, dz, 256, 1), row_part(wpo, dz, 256, 0))
    for line in s_lines:
        relay_far(line)
    s_lines[0].own.arrive_all(sbuf.at[:, 0 : 3 * 128])
    s_lines[0].cross_far.arrive_all(sbuf.at[:, 0:128])
    for dz in (0, 1, -1):
        total = total + dot(row_part(sbuf, dz, 256, 1), row_part(wst, dz, 256, 0))
    w_out.ready(2)
    total = total + dot(row_part(pbuf, 2, 256, 1), row_part(wpo, 2, 256, 0))
    total = total + dot(row_part(sbuf, 2, 256, 1), row_part(wst, 2, 256, 0))
    out[...] = total.astype(BF16)

    one.own.left_all(tok.at[:, 0 : 7 * FEATURES])
    for plane, refs in ((w_in, (win.at[0:1440], win.at[0:1440])), (w_out, (wst.at[0:960], wpo.at[0:960]))):
        plane.a[0].left_all(refs[0])
        plane.b[0].left_all(refs[1])
    moves[0].left_all(ends.at[0 : PEERS - 1])
    pline.own.left_all(pbuf.at[:, 0:896])
    s_lines[0].own.left_all(sbuf.at[:, 0:896])
    halo_move.left_all(halo.at[0])


def body(
    tokens, norm_gain, state_in_weight, pool_in_weight, rate_real, rate_imag, log_step, input_real, input_imag,
    output_real, output_imag, skip_gain, pool_weight, pool_gain, state_out_weight, pool_out_weight,
):
    vmem = pl.BlockSpec(memory_space=pltpu.VMEM)
    dma = pltpu.SemaphoreType.DMA
    return pl.pallas_call(
        kernel,
        out_shape=pltpu.VMEM((ROWS, FEATURES), BF16),
        in_specs=[pl.BlockSpec(memory_space=pltpu.HBM)] * 16,
        out_specs=vmem,
        scratch_shapes=[
            pltpu.VMEM((1, 3072), F32),
            pltpu.VMEM((GROUPS, STATE), F32),
            pltpu.VMEM((GROUPS, STATE), F32),
            pltpu.VMEM((1, 64), F32),
            pltpu.VMEM((1, 128), F32),
            pltpu.VMEM((1, 128), F32),
            pltpu.VMEM((ROWS, FEATURES), BF16),
            pltpu.VMEM((ROWS, 3072), BF16),
            pltpu.VMEM((ROWS, 3072), BF16),
            pltpu.VMEM((3072, 256), BF16),
            pltpu.VMEM((1024, FEATURES), BF16),
            pltpu.VMEM((1024, FEATURES), BF16),
            pltpu.VMEM((GROUPS, CHANNEL, STATE), F32),
            pltpu.VMEM((GROUPS, CHANNEL, STATE), F32),
            pltpu.VMEM((GROUPS, CHANNEL, STATE), F32),
            pltpu.VMEM((GROUPS, CHANNEL, STATE), F32),
            pltpu.VMEM((2, 64, 64), BF16),
            pltpu.VMEM((256, 2 * WIDTH), BF16),
            pltpu.VMEM((2 * WIDTH, 256), BF16),
            pltpu.VMEM((ROWS, ROWS), BF16),
            pltpu.VMEM((2 * ROWS, ROWS), BF16),
            pltpu.VMEM((2 * ROWS, REACH), BF16),
            pltpu.VMEM((ROWS, 128), F32),
            pltpu.VMEM((ROWS, 2 * WIDTH), F32),
            pltpu.VMEM((ROWS, 2 * WIDTH), BF16),
            pltpu.VMEM((ROWS, 2 * WIDTH), BF16),
            pltpu.VMEM((PEERS, 8, 128), F32),
            pltpu.VMEM((PEERS, REACH, 128), BF16),
            pltpu.VMEM((ROWS, 1024), BF16),
            pltpu.VMEM((ROWS, 1024), BF16),
            dma((16,)), dma((1,)), dma((8,)), dma((2,)), dma((24,)), dma((2,)), dma((24,)),
            pltpu.SemaphoreType.REGULAR, dma((1,)), dma((1,)), dma((1,)), dma((1,)),
            dma((1,)), dma((8,)), dma((1,)), dma((4,)),
        ],
        compiler_params=pltpu.CompilerParams(collective_id=0, has_side_effects=True, vmem_limit_bytes=60000000),
    )(*(pltpu.with_memory_space_constraint(v, pltpu.HBM) for v in (
        tokens, norm_gain.reshape(1, 3072), state_in_weight, pool_in_weight, rate_real, rate_imag,
        log_step.reshape(1, 64), jnp.swapaxes(input_real, 1, 2), jnp.swapaxes(input_imag, 1, 2), output_real, output_imag, skip_gain.reshape(1, 1024),
        pool_weight, pool_gain.reshape(1, 1024), state_out_weight, pool_out_weight,
    )))


def solution(mesh):
    tile = P("sp", "tp")
    in_specs = (tile, P(), tile, tile, *(P() for _ in range(10)), tile, tile)
    return jax.shard_map(body, mesh=mesh, in_specs=in_specs, out_specs=tile, check_vma=False)
```

```python
import functools

import jax
import jax.numpy as jnp
from jax import lax
from jax.experimental import pallas as pl
from jax.experimental.pallas import tpu as pltpu
from jax.sharding import PartitionSpec as P

EPSILON = 1e-06
HIGHEST = lax.Precision.HIGHEST
MESH = pl.DeviceIdType.MESH
F32, BF16 = jnp.float32, jnp.bfloat16

ROWS = 256
STEPS, PARTS = 32, 8
FEATURES = 384
PEERS, HEADS_TP = 16, 8
GROUPS, STATE, CHANNEL = 8, 64, 16
WIDTH = GROUPS * STATE
REACH = 16


def iota(shape, dim):
    return lax.broadcasted_iota(jnp.int32, shape, dim)


def position_of(row):
    return STEPS * (row % PARTS) + row // PARTS


def dot(a, b, precision=None):
    return jnp.dot(a, b, preferred_element_type=F32, precision=precision)


def split(value):
    high = value.astype(BF16)
    return high, (value - high.astype(F32)).astype(BF16)


class Move:
    def __init__(self, sends, fills, device, send_sem, recv_sem):
        self.sends, self.fills, self.device, self.send_sem, self.recv_sem = sends, fills, device, send_sem, recv_sem

    def copy(self, ref):
        return pltpu.make_async_remote_copy(
            src_ref=ref, dst_ref=ref, send_sem=self.send_sem, recv_sem=self.recv_sem,
            device_id=self.device, device_id_type=MESH)

    def start(self):
        self.copy(self.sends).start()

    def arrive(self):
        self.copy(self.fills).wait_recv()

    def arrive_all(self, ref):
        self.copy(ref).wait_recv()

    def left_all(self, ref):
        self.copy(ref).wait_send()


class LineGather:
    def __init__(self, slot, sems, first, shared, y, c, across):
        d = 1 - 2 * c
        at = lambda k, core: slot(lax.rem(y + k + 4, 4) * 2 + core)
        to = lambda k, core: {"tp": lax.rem(y + k + 4, 4) * 2 + core}
        o = 1 - c
        places = [first, first + 1, first + 2, shared[0], shared[0], shared[0], shared[1]]
        mk = lambda s, f, dev, i: Move(s, f, dev, sems[0].at[0], sems[1].at[places[i]])
        self.ahead = mk(at(0, c), at(-d, c), to(d, c), 0)
        self.back = mk(at(0, c), at(d, c), to(-d, c), 1)
        self.onward = mk(at(-d, c), at(-2 * d, c), to(d, c), 2)
        self.own = mk(at(0, c), at(0, o), to(0, o), 3)
        self.cross_ahead = mk(at(-d, c), at(d, o), to(0, o), 4)
        self.cross_back = mk(at(d, c), at(-d, o), to(0, o), 5)
        self.across = across
        self.cross_far = mk(at(-d, c) if across else at(-2 * d, c), at(2 * d, o), to(d if across else 0, o), 6)
        self.all = [self.ahead, self.back, self.onward, self.own, self.cross_ahead, self.cross_back, self.cross_far]
        index = lambda k, core: lax.rem(y + k + 4, 4) * 2 + core
        self.index = dict(own=index(0, c), ahead=index(-d, c), back=index(d, c), onward=index(-2 * d, c),
                          p_own=index(0, o), p_ahead=index(d, o), p_back=index(-d, o), p_onward=index(2 * d, o))


class PlaneGather:
    def __init__(self, slot_a, slot_b, sems, sized, z, x):
        wrap = lambda k: lax.rem(k + 4, 4)
        at = lambda dz, dx: wrap(z + dz) * 4 + wrap(x + dx)
        self.count, self.sized, self.groups, self.places = 0, sized, {}, {}

        def mk(half, sent, filled, device, key=None):
            slot = (slot_a, slot_b)[half]
            place = self.places.get(key, self.count)
            if place == self.count:
                self.count += 1
            move = Move(slot(at(*sent)), slot(at(*filled)), {"sp": at(*device)}, sems[0].at[half], sems[1].at[place])
            if key is not None:
                self.places[key] = place
                self.groups.setdefault(key, []).append(move)
            return move

        def ring(half, along, e, base):
            v = (lambda k: (base, k)) if along == "x" else (lambda k: (k, base))
            w = (lambda k: (0, k)) if along == "x" else (lambda k: (k, 0))
            key = lambda k: (half, base if along == "x" else k)
            return [
                mk(half, v(0), v(-e), w(e)),
                mk(half, v(0), v(e), w(-e), key(e)),
                mk(half, v(-e), v(-2 * e), w(e), key(2)),
            ]

        self.a = [mk(0, (0, 0), (0, -k), (0, k)) for k in (1, -1, 2)]
        self.b = [mk(1, (0, 0), (-k, 0), (k, 0)) for k in (-1, 1, 2)]
        heavy = {0: 1, -1: -1, 1: -1, 2: 1}
        self.za = {o: ring(0, "z", heavy[o], o) for o in (0, -1, 1, 2)}
        self.xb = {o: ring(1, "x", -heavy[o], o) for o in (0, -1, 1, 2)}

    def ready(self, dz):
        for half in (0, 1):
            group = self.groups.get((half, dz), [])
            if group:
                group[0].arrive_all(self.sized(half, len(group)))

    def begin(self):
        for ring in (self.a, self.b):
            ring[0].start()
            ring[1].start()
        for ring in (self.a, self.b):
            ring[2].start()
        for ring in (self.za[0], self.xb[0]):
            ring[0].start()
            ring[1].start()

    def events(self):
        def across(move, ring, count):
            def event():
                move.arrive()
                for k in range(count):
                    ring[k].start()
            return event

        def onward(ring):
            def event():
                ring[0].arrive()
                ring[2].start()
            return event

        return [
            across(self.a[0], self.za[-1], 2), across(self.b[0], self.xb[1], 2),
            across(self.a[1], self.za[1], 2), across(self.b[1], self.xb[-1], 2),
            across(self.a[2], self.za[2], 2), across(self.b[2], self.xb[2], 2),
            onward(self.za[0]), onward(self.xb[0]),
            onward(self.za[-1]), onward(self.xb[1]), onward(self.za[1]), onward(self.xb[-1]),
            onward(self.za[2]), onward(self.xb[2]),
        ]


def kernel(
    tokens, gain_all, state_in_w, pool_in_w, rate_real_all, rate_imag_all, log_step_all, input_real, input_imag,
    output_real, output_imag, skip_all, pool_weight, pool_gain_all, state_out_w, pool_out_w, out,
    gain, rate_real, rate_imag, log_step, skip_gain, pool_gain, own_tokens, tok, scaled, win, wst, wpo, in_re, in_im, out_re, out_im, mix_raw,
    drive, read, unsort, bands, tails, recip, push, high, low, ends, halo, sbuf, pbuf,
    local_sem, tok_send, tok_recv, win_send, win_recv, wout_send, wout_recv,
    ready, end_send, end_recv, halo_send, halo_recv, s_send, s_recv, p_send, p_recv,
):
    s, t = lax.axis_index("sp"), lax.axis_index("tp")
    z, x, y, c = s // 4, s % 4, t // 2, t % 2
    g0 = t * GROUPS

    def lanes(ref, index, width):
        return ref.at[:, pl.ds(pl.multiple_of(index * width, 128), width)]

    def rows(ref, start, count):
        return ref.at[pl.ds(pl.multiple_of(start, 16), count), :]

    loads = [
        (tokens, own_tokens),
        (state_in_w, win.at[pl.ds(pl.multiple_of(s * 192, 16), 192), 0:128]),
        (pool_in_w, win.at[pl.ds(pl.multiple_of(s * 192, 16), 192), 128:256]),
        (state_out_w, rows(wst, s * 64, 64)),
        (pool_out_w, rows(wpo, s * 64, 64)),
        (input_real.at[pl.ds(g0, GROUPS)], in_re),
        (input_imag.at[pl.ds(g0, GROUPS)], in_im),
        (output_real.at[pl.ds(g0, GROUPS)], out_re),
        (output_imag.at[pl.ds(g0, GROUPS)], out_im),
        (pool_weight.at[pl.ds(2 * t, 2)], mix_raw),
        (gain_all, gain),
        (rate_real_all.at[pl.ds(pl.multiple_of(g0, 8), GROUPS), :], rate_real),
        (rate_imag_all.at[pl.ds(pl.multiple_of(g0, 8), GROUPS), :], rate_imag),
        (log_step_all, log_step),
        (lanes(skip_all, t, 128), skip_gain),
        (lanes(pool_gain_all, t, 128), pool_gain),
    ]
    loads = [pltpu.make_async_copy(a, b, local_sem.at[k]) for k, (a, b) in enumerate(loads)]
    for load in loads:
        load.start()

    barrier = pltpu.get_barrier_semaphore()
    beside = [z * 4 + lax.rem(x + k, 4) for k in (1, 2, 3)]
    above = [lax.rem(z + k, 4) * 4 + x for k in (1, 2, 3)]
    for peer in (*beside, *above):
        pl.semaphore_signal(barrier, inc=1, device_id={"sp": peer}, device_id_type=MESH)
    for k in range(1, HEADS_TP):
        pl.semaphore_signal(barrier, inc=1, device_id={"tp": lax.rem(t + k, HEADS_TP)}, device_id_type=MESH)

    r0, r1 = iota((ROWS, ROWS), 0), iota((ROWS, ROWS), 1)
    loads[0].wait()
    sort = (position_of(r0) == r1).astype(BF16)
    lanes(tok, t, FEATURES)[...] = dot(sort, own_tokens[...]).astype(BF16)
    unsort[...] = (position_of(r1) == r0).astype(BF16)

    def halves(ref, width, sems, across):
        def of(k):
            return lambda p: ref.at[pl.ds(k * 128, 128), pl.ds(pl.multiple_of(p * width, 128), width)]
        return [LineGather(of(k), sems, 3 * k, (6, 7), y, c, across) for k in range(2)]

    tok_lines = halves(tok, FEATURES, (tok_send, tok_recv), False)
    w_in = PlaneGather(
        lambda q: rows(win, q * 192, 96), lambda q: rows(win, q * 192 + 96, 96), (win_send, win_recv),
        lambda half, n: win.at[0 : 96 * n], z, x)
    w_out = PlaneGather(
        lambda q: rows(wst, q * 64, 64), lambda q: rows(wpo, q * 64, 64), (wout_send, wout_recv),
        lambda half, n: (wst, wpo)[half].at[0 : 64 * n], z, x)
    pl.semaphore_wait(barrier, 6 + HEADS_TP - 1)
    for line in tok_lines:
        line.ahead.start()
        line.back.start()
    for load in loads[1:3]:
        load.wait()
    w_in.begin()
    for line in tok_lines:
        line.own.start()
    for peer in beside:
        pl.semaphore_signal(ready, inc=1, device_id={"sp": peer}, device_id_type=MESH)
    for load in loads[3:]:
        load.wait()

    wanted = iota((GROUPS, STATE), 0) + g0
    steps_log = jnp.sum(jnp.where(iota((GROUPS, 64), 1) == wanted, log_step[...], 0.0), axis=1, keepdims=True)
    step = jnp.exp(steps_log) / float(ROWS * PEERS)
    real = rate_real[...]
    imag = rate_imag[...]
    exponent, angle = real * step, imag * step
    magnitude = jnp.exp(exponent)
    cosine, sine, half_sine = jnp.cos(angle), jnp.sin(angle), jnp.sin(0.5 * angle)
    decay_real, decay_imag = magnitude * cosine, magnitude * sine
    less = exponent * (1.0 + exponent * 0.5 * (1.0 + exponent * (1.0 / 3.0) * (1.0 + exponent * 0.25)))
    less = less * cosine - 2.0 * half_sine * half_sine
    denominator = real * real + imag * imag
    factor_real = (less * real + decay_imag * imag) / denominator
    factor_imag = (decay_imag * real - less * imag) / denominator

    spread = (iota((STATE, WIDTH), 1) % STATE == iota((STATE, WIDTH), 0)).astype(F32)
    own_group = iota((GROUPS, WIDTH), 1) // STATE == iota((GROUPS, WIDTH), 0)

    def flat(value):
        return jnp.sum(jnp.where(own_group, dot(value, spread, HIGHEST), 0.0), axis=0, keepdims=True)

    lr, li = flat(decay_real), flat(decay_imag)
    fr, fi = flat(factor_real), flat(factor_imag)

    def times(ar, ai, br, bi):
        return ar * br - ai * bi, ar * bi + ai * br

    pr, pi = lr, li
    for _ in range(5):
        pr, pi = times(pr, pi, pr, pi)
    part_real, part_imag = pr, pi
    for _ in range(3):
        pr, pi = times(pr, pi, pr, pi)
    block_real, block_imag = pr, pi
    sub = iota((PARTS, WIDTH), 0)
    up_real, up_imag = jnp.ones((PARTS, WIDTH), F32), jnp.zeros((PARTS, WIDTH), F32)
    down_real, down_imag = up_real, up_imag
    wr, wi = jnp.ones((1, WIDTH), F32), jnp.zeros((1, WIDTH), F32)
    for k in range(1, PARTS):
        wr, wi = times(wr, wi, part_real, part_imag)
        up_real, up_imag = jnp.where(sub == k, wr, up_real), jnp.where(sub == k, wi, up_imag)
        down_real = jnp.where(sub == PARTS - 1 - k, wr, down_real)
        down_imag = jnp.where(sub == PARTS - 1 - k, wi, down_imag)

    own_read = iota((128, WIDTH), 0) // CHANNEL == iota((128, WIDTH), 1) // STATE
    for k, ref in enumerate((in_re, in_im)):
        wide = jnp.where(own_read, dot(ref[...].reshape(128, STATE), spread, HIGHEST), 0.0)
        top, rest = split(wide)
        drive[0:128, k * WIDTH : (k + 1) * WIDTH] = top
        drive[128:256, k * WIDTH : (k + 1) * WIDTH] = rest
    cr = jnp.where(own_read, dot(out_re[...].reshape(128, STATE), spread, HIGHEST), 0.0)
    ci = jnp.where(own_read, dot(out_im[...].reshape(128, STATE), spread, HIGHEST), 0.0)
    for k, part in enumerate((cr * fr - ci * fi, -(cr * fi + ci * fr))):
        top, rest = split(jnp.transpose(part))
        read[k * WIDTH : (k + 1) * WIDTH, 0:128] = top
        read[k * WIDTH : (k + 1) * WIDTH, 128:256] = rest

    window0 = jnp.where(c == 0, 2, 8)
    p0, p1 = position_of(r0), position_of(r1)
    for k in range(2):
        w = window0 * (k + 1)
        bands[k * ROWS : (k + 1) * ROWS, :] = ((p1 <= p0) & (p1 > p0 - w)).astype(BF16)
        h0, h1 = position_of(iota((ROWS, REACH), 0)), iota((ROWS, REACH), 1) - REACH
        tails[k * ROWS : (k + 1) * ROWS, :] = (h1 > h0 - w).astype(BF16)
    first_head = iota((ROWS, 128), 1) < 64
    here = position_of(iota((ROWS, 128), 0)) + s * ROWS + 1
    recip[...] = 1.0 / jnp.minimum(here, jnp.where(first_head, window0, 2 * window0)).astype(F32)
    last = (position_of(iota((REACH, ROWS), 1)) == iota((REACH, ROWS), 0) + (ROWS - REACH)).astype(BF16)

    pair = (iota((64, 128), 1) % 64 == iota((64, 128), 0)).astype(BF16)
    mixer = jnp.where(
        iota((128, 128), 0) // 64 == iota((128, 128), 1) // 64, dot(mix_raw[...].reshape(128, 64), pair), 0.0
    ).astype(BF16)

    def prepare(p, squares):
        ref = lanes(tok, p, FEATURES)
        f = ref[...].astype(F32)
        lanes(scaled, p, FEATURES)[...] = (f * gain[:, pl.ds(pl.multiple_of(p * FEATURES, 128), FEATURES)]).astype(BF16)
        f = f * f
        return squares + (f[:, 0:128] + f[:, 128:256] + f[:, 256:384])

    squares = prepare(t, jnp.zeros((ROWS, 128), F32))

    def relay(line):
        line.ahead.arrive()
        line.onward.start()
        if line.across:
            line.cross_far.start()
        line.cross_ahead.start()
        line.back.arrive()
        line.cross_back.start()

    def relay_far(line):
        line.onward.arrive()
        if not line.across:
            line.cross_far.start()

    events, later = w_in.events(), w_out.events()
    one, two = tok_lines
    index = one.index

    def run(which, first, last):
        for e in which[first:last]:
            e()

    run(events, 0, 4)
    relay(one)
    run(events, 4, 8)
    relay(two)
    run(events, 8, 14)
    w_out.begin()
    relay_far(one)
    for name in ("ahead", "back"):
        squares = prepare(index[name], squares)
    relay_far(two)
    squares = prepare(index["onward"], squares)
    one.own.arrive_all(tok.at[:, 0 : 3 * FEATURES])
    for name in ("p_own", "p_ahead", "p_back"):
        squares = prepare(index[name], squares)
    one.cross_far.arrive_all(tok.at[:, 0:FEATURES])
    squares = prepare(index["p_onward"], squares)
    inverse = lax.rsqrt(jnp.sum(squares, axis=1, keepdims=True) / 3072.0 + EPSILON)

    def row_part(ref, dz, width, axis):
        at = pl.ds(pl.multiple_of(lax.rem(z + dz + 4, 4) * width, 128), width)
        return ref[:, at] if axis else ref[at, :]

    product = jnp.zeros((ROWS, 256), F32)
    for dz in (0, 1, -1, 2):
        w_in.ready(dz)
        product = product + dot(row_part(scaled, dz, 768, 1), row_part(win, dz, 768, 0))
    entry = (product * inverse).astype(BF16)
    state_in, pool_in = entry[:, 0:128], entry[:, 128:256]

    pl.semaphore_wait(ready, 3)
    halo[s] = dot(last, pool_in).astype(BF16)
    back = lax.rem(s + PEERS - 1, PEERS)
    halo_move = Move(halo.at[s], halo.at[back], {"sp": lax.rem(s + 1, PEERS)}, halo_send.at[0], halo_recv.at[0])
    halo_move.start()

    push[...] = dot(jnp.concatenate([state_in, state_in], axis=1), drive[...])
    lrb, lib = jnp.broadcast_to(lr, (PARTS, WIDTH)), jnp.broadcast_to(li, (PARTS, WIDTH))

    def advance(j, carry):
        sr, si = carry
        at = pl.ds(pl.multiple_of(j * PARTS, PARTS), PARTS)
        nr = lrb * sr - lib * si + push[at, 0:WIDTH]
        ni = lrb * si + lib * sr + push[at, WIDTH : 2 * WIDTH]
        return nr, ni

    zero = jnp.zeros((PARTS, WIDTH), F32)
    er, ei = lax.fori_loop(0, STEPS, advance, (zero, zero), unroll=8)
    br, bi = times(er, ei, down_real, down_imag)
    br, bi = jnp.sum(br, axis=0, keepdims=True), jnp.sum(bi, axis=0, keepdims=True)
    lines = lambda row: [row[:, 128 * k : 128 * (k + 1)] for k in range(WIDTH // 128)]
    ends[s] = jnp.concatenate(lines(br) + lines(bi), axis=0)
    block = lambda dz, dx: lax.rem(z + dz + 4, 4) * 4 + lax.rem(x + dx + 4, 4)
    offsets = [(dz, dx) for dz in (2, 1, -1, 0) for dx in (2, 1, -1, 0)][:-1]
    farthest_first = sorted(offsets, key=lambda o: -abs(o[0]) - abs(o[1]))
    moves = [
        Move(ends.at[s], ends.at[block(-dz, -dx)], {"sp": block(dz, dx)}, end_send.at[0], end_recv.at[0])
        for dz, dx in farthest_first
    ]
    for m in moves:
        m.start()

    sums = dot(bands[...], pool_in)
    halo_move.arrive()
    before = halo[back]
    before = jnp.where(s > 0, before.astype(F32), 0.0).astype(BF16)
    sums = sums + dot(tails[...], before)
    pooled = jnp.where(first_head, sums[0:ROWS], sums[ROWS : 2 * ROWS]) * recip[...] - pool_in.astype(F32)
    top, rest = split(pooled)
    projected = dot(top, mixer) + dot(rest, mixer)
    pool_out = (projected * pool_gain[...]).astype(BF16)
    lanes(pbuf, t, 128)[...] = dot(unsort[...], pool_out).astype(BF16)
    pline = LineGather(lambda p: lanes(pbuf, p, 128), (p_send, p_recv), 0, (3, 3), y, c, True)
    pline.ahead.start()
    pline.back.start()
    pline.own.start()

    kr, ki = jnp.where(sub >= 1, pltpu.roll(er, 1, 0), 0.0), jnp.where(sub >= 1, pltpu.roll(ei, 1, 0), 0.0)
    gr, gi = part_real, part_imag
    for hop in (1, 2, 4):
        tr = jnp.where(sub >= hop, pltpu.roll(kr, hop, 0), 0.0)
        ti = jnp.where(sub >= hop, pltpu.roll(ki, hop, 0), 0.0)
        ar, ai = times(tr, ti, gr, gi)
        kr, ki = kr + ar, ki + ai
        gr, gi = times(gr, gi, gr, gi)

    run(later, 0, 6)
    moves[0].arrive_all(ends.at[0 : PEERS - 1])
    qr = jnp.concatenate(lines(block_real), axis=0)
    qi = jnp.concatenate(lines(block_imag), axis=0)
    hr, hi = jnp.zeros_like(qr), jnp.zeros_like(qi)
    for q in range(PEERS - 1):
        piece = ends[q]
        ar, ai = times(hr, hi, qr, qi)
        hr, hi = jnp.where(q < s, ar + piece[0:4], hr), jnp.where(q < s, ai + piece[4:8], hi)
    hr = jnp.concatenate([hr[k : k + 1] for k in range(4)], axis=1)
    hi = jnp.concatenate([hi[k : k + 1] for k in range(4)], axis=1)
    ar, ai = times(up_real, up_imag, hr, hi)

    def advance_pair(j, carry):
        one = advance(2 * j, carry)
        two = advance(2 * j + 1, one)
        at = pl.ds(pl.multiple_of(j * 2 * PARTS, 2 * PARTS), 2 * PARTS)
        for k in range(2):
            top, rest = split(jnp.concatenate([one[k], two[k]], axis=0))
            high[at, k * WIDTH : (k + 1) * WIDTH] = top
            low[at, k * WIDTH : (k + 1) * WIDTH] = rest
        return two

    lax.fori_loop(0, STEPS // 2, advance_pair, (kr + ar, ki + ai), unroll=4)
    both = dot(high[...], read[...])
    readout = both[:, 0:128] + both[:, 128:256] + dot(low[...], read[:, 0:128])
    readout = readout + skip_gain[...] * state_in.astype(F32)
    state_out = jax.nn.gelu(readout).astype(BF16)
    lanes(sbuf, t, 128)[...] = dot(unsort[...], state_out).astype(BF16)
    s_lines = halves(sbuf, 128, (s_send, s_recv), True)
    for line in s_lines:
        line.ahead.start()
        line.back.start()
    for line in s_lines:
        line.own.start()
    relay(pline)
    for line in s_lines:
        relay(line)
    run(later, 6, 14)
    relay_far(pline)
    pline.own.arrive_all(pbuf.at[:, 0:512])
    total = jnp.zeros((ROWS, FEATURES), F32)
    for dz in (0, 1, -1):
        w_out.ready(dz)
        total = total + dot(row_part(pbuf, dz, 256, 1), row_part(wpo, dz, 256, 0))
    for line in s_lines:
        relay_far(line)
    s_lines[0].own.arrive_all(sbuf.at[:, 0 : 3 * 128])
    s_lines[0].cross_far.arrive_all(sbuf.at[:, 0:128])
    for dz in (0, 1, -1):
        total = total + dot(row_part(sbuf, dz, 256, 1), row_part(wst, dz, 256, 0))
    w_out.ready(2)
    total = total + dot(row_part(pbuf, 2, 256, 1), row_part(wpo, 2, 256, 0))
    total = total + dot(row_part(sbuf, 2, 256, 1), row_part(wst, 2, 256, 0))
    out[...] = total.astype(BF16)

    one.own.left_all(tok.at[:, 0 : 7 * FEATURES])
    for plane, refs in ((w_in, (win.at[0:1440], win.at[0:1440])), (w_out, (wst.at[0:960], wpo.at[0:960]))):
        plane.a[0].left_all(refs[0])
        plane.b[0].left_all(refs[1])
    moves[0].left_all(ends.at[0 : PEERS - 1])
    pline.own.left_all(pbuf.at[:, 0:896])
    s_lines[0].own.left_all(sbuf.at[:, 0:896])
    halo_move.left_all(halo.at[0])


def body(
    tokens, norm_gain, state_in_weight, pool_in_weight, rate_real, rate_imag, log_step, input_real, input_imag,
    output_real, output_imag, skip_gain, pool_weight, pool_gain, state_out_weight, pool_out_weight,
):
    vmem = pl.BlockSpec(memory_space=pltpu.VMEM)
    dma = pltpu.SemaphoreType.DMA
    return pl.pallas_call(
        kernel,
        out_shape=pltpu.VMEM((ROWS, FEATURES), BF16),
        in_specs=[pl.BlockSpec(memory_space=pltpu.HBM)] * 16,
        out_specs=vmem,
        scratch_shapes=[
            pltpu.VMEM((1, 3072), F32),
            pltpu.VMEM((GROUPS, STATE), F32),
            pltpu.VMEM((GROUPS, STATE), F32),
            pltpu.VMEM((1, 64), F32),
            pltpu.VMEM((1, 128), F32),
            pltpu.VMEM((1, 128), F32),
            pltpu.VMEM((ROWS, FEATURES), BF16),
            pltpu.VMEM((ROWS, 3072), BF16),
            pltpu.VMEM((ROWS, 3072), BF16),
            pltpu.VMEM((3072, 256), BF16),
            pltpu.VMEM((1024, FEATURES), BF16),
            pltpu.VMEM((1024, FEATURES), BF16),
            pltpu.VMEM((GROUPS, CHANNEL, STATE), F32),
            pltpu.VMEM((GROUPS, CHANNEL, STATE), F32),
            pltpu.VMEM((GROUPS, CHANNEL, STATE), F32),
            pltpu.VMEM((GROUPS, CHANNEL, STATE), F32),
            pltpu.VMEM((2, 64, 64), BF16),
            pltpu.VMEM((256, 2 * WIDTH), BF16),
            pltpu.VMEM((2 * WIDTH, 256), BF16),
            pltpu.VMEM((ROWS, ROWS), BF16),
            pltpu.VMEM((2 * ROWS, ROWS), BF16),
            pltpu.VMEM((2 * ROWS, REACH), BF16),
            pltpu.VMEM((ROWS, 128), F32),
            pltpu.VMEM((ROWS, 2 * WIDTH), F32),
            pltpu.VMEM((ROWS, 2 * WIDTH), BF16),
            pltpu.VMEM((ROWS, 2 * WIDTH), BF16),
            pltpu.VMEM((PEERS, 8, 128), F32),
            pltpu.VMEM((PEERS, REACH, 128), BF16),
            pltpu.VMEM((ROWS, 1024), BF16),
            pltpu.VMEM((ROWS, 1024), BF16),
            dma((16,)), dma((1,)), dma((8,)), dma((2,)), dma((24,)), dma((2,)), dma((24,)),
            pltpu.SemaphoreType.REGULAR, dma((1,)), dma((1,)), dma((1,)), dma((1,)),
            dma((1,)), dma((8,)), dma((1,)), dma((4,)),
        ],
        compiler_params=pltpu.CompilerParams(collective_id=0, has_side_effects=True, vmem_limit_bytes=60000000),
    )(*(pltpu.with_memory_space_constraint(v, pltpu.HBM) for v in (
        tokens, norm_gain.reshape(1, 3072), state_in_weight, pool_in_weight, rate_real, rate_imag,
        log_step.reshape(1, 64), jnp.swapaxes(input_real, 1, 2), jnp.swapaxes(input_imag, 1, 2), output_real, output_imag, skip_gain.reshape(1, 1024),
        pool_weight, pool_gain.reshape(1, 1024), state_out_weight, pool_out_weight,
    )))


def solution(mesh):
    tile = P("sp", "tp")
    in_specs = (tile, P(), tile, tile, *(P() for _ in range(10)), tile, tile)
    return jax.shard_map(body, mesh=mesh, in_specs=in_specs, out_specs=tile, check_vma=False)
```

```python
import functools

import jax
import jax.numpy as jnp
from jax import lax
from jax.experimental import pallas as pl
from jax.experimental.pallas import tpu as pltpu
from jax.sharding import PartitionSpec as P

EPSILON = 1e-06
HIGHEST = lax.Precision.HIGHEST
MESH = pl.DeviceIdType.MESH
F32, BF16 = jnp.float32, jnp.bfloat16

ROWS = 256
STEPS, PARTS = 32, 8
FEATURES = 384
PEERS, HEADS_TP = 16, 8
GROUPS, STATE, CHANNEL = 8, 64, 16
WIDTH = GROUPS * STATE
REACH = 16


def iota(shape, dim):
    return lax.broadcasted_iota(jnp.int32, shape, dim)


def position_of(row):
    return STEPS * (row % PARTS) + row // PARTS


def dot(a, b, precision=None):
    return jnp.dot(a, b, preferred_element_type=F32, precision=precision)


def split(value):
    high = value.astype(BF16)
    return high, (value - high.astype(F32)).astype(BF16)


class Move:
    def __init__(self, sends, fills, device, send_sem, recv_sem):
        self.sends, self.fills, self.device, self.send_sem, self.recv_sem = sends, fills, device, send_sem, recv_sem

    def copy(self, ref):
        return pltpu.make_async_remote_copy(
            src_ref=ref, dst_ref=ref, send_sem=self.send_sem, recv_sem=self.recv_sem,
            device_id=self.device, device_id_type=MESH)

    def start(self):
        self.copy(self.sends).start()

    def arrive(self):
        self.copy(self.fills).wait_recv()

    def arrive_all(self, ref):
        self.copy(ref).wait_recv()

    def left_all(self, ref):
        self.copy(ref).wait_send()


class LineGather:
    def __init__(self, slot, sems, first, shared, y, c, across):
        d = 1 - 2 * c
        at = lambda k, core: slot(lax.rem(y + k + 4, 4) * 2 + core)
        to = lambda k, core: {"tp": lax.rem(y + k + 4, 4) * 2 + core}
        o = 1 - c
        places = [first, first + 1, first + 2, shared[0], shared[0], shared[0], shared[1]]
        mk = lambda s, f, dev, i: Move(s, f, dev, sems[0].at[0], sems[1].at[places[i]])
        self.ahead = mk(at(0, c), at(-d, c), to(d, c), 0)
        self.back = mk(at(0, c), at(d, c), to(-d, c), 1)
        self.onward = mk(at(-d, c), at(-2 * d, c), to(d, c), 2)
        self.own = mk(at(0, c), at(0, o), to(0, o), 3)
        self.cross_ahead = mk(at(-d, c), at(d, o), to(0, o), 4)
        self.cross_back = mk(at(d, c), at(-d, o), to(0, o), 5)
        self.across = across
        self.cross_far = mk(at(-d, c) if across else at(-2 * d, c), at(2 * d, o), to(d if across else 0, o), 6)
        self.all = [self.ahead, self.back, self.onward, self.own, self.cross_ahead, self.cross_back, self.cross_far]
        index = lambda k, core: lax.rem(y + k + 4, 4) * 2 + core
        self.index = dict(own=index(0, c), ahead=index(-d, c), back=index(d, c), onward=index(-2 * d, c),
                          p_own=index(0, o), p_ahead=index(d, o), p_back=index(-d, o), p_onward=index(2 * d, o))


class PlaneGather:
    def __init__(self, slot_a, slot_b, sems, sized, z, x):
        wrap = lambda k: lax.rem(k + 4, 4)
        at = lambda dz, dx: wrap(z + dz) * 4 + wrap(x + dx)
        self.count, self.sized, self.groups, self.places = 0, sized, {}, {}

        def mk(half, sent, filled, device, key=None):
            slot = (slot_a, slot_b)[half]
            place = self.places.get(key, self.count)
            if place == self.count:
                self.count += 1
            move = Move(slot(at(*sent)), slot(at(*filled)), {"sp": at(*device)}, sems[0].at[half], sems[1].at[place])
            if key is not None:
                self.places[key] = place
                self.groups.setdefault(key, []).append(move)
            return move

        def ring(half, along, e, base):
            v = (lambda k: (base, k)) if along == "x" else (lambda k: (k, base))
            w = (lambda k: (0, k)) if along == "x" else (lambda k: (k, 0))
            key = lambda k: (half, base if along == "x" else k)
            return [
                mk(half, v(0), v(-e), w(e)),
                mk(half, v(0), v(e), w(-e), key(e)),
                mk(half, v(-e), v(-2 * e), w(e), key(2)),
            ]

        self.a = [mk(0, (0, 0), (0, -k), (0, k)) for k in (1, -1, 2)]
        self.b = [mk(1, (0, 0), (-k, 0), (k, 0)) for k in (-1, 1, 2)]
        heavy = {0: 1, -1: -1, 1: -1, 2: 1}
        self.za = {o: ring(0, "z", heavy[o], o) for o in (0, -1, 1, 2)}
        self.xb = {o: ring(1, "x", -heavy[o], o) for o in (0, -1, 1, 2)}

    def ready(self, dz):
        for half in (0, 1):
            group = self.groups.get((half, dz), [])
            if group:
                group[0].arrive_all(self.sized(half, len(group)))

    def begin(self):
        for ring in (self.a, self.b):
            ring[0].start()
            ring[1].start()
        for ring in (self.a, self.b):
            ring[2].start()
        for ring in (self.za[0], self.xb[0]):
            ring[0].start()
            ring[1].start()

    def events(self):
        def across(move, ring, count):
            def event():
                move.arrive()
                for k in range(count):
                    ring[k].start()
            return event

        def onward(ring):
            def event():
                ring[0].arrive()
                ring[2].start()
            return event

        return [
            across(self.a[0], self.za[-1], 2), across(self.b[0], self.xb[1], 2),
            across(self.a[1], self.za[1], 2), across(self.b[1], self.xb[-1], 2),
            across(self.a[2], self.za[2], 2), across(self.b[2], self.xb[2], 2),
            onward(self.za[0]), onward(self.xb[0]),
            onward(self.za[-1]), onward(self.xb[1]), onward(self.za[1]), onward(self.xb[-1]),
            onward(self.za[2]), onward(self.xb[2]),
        ]


def kernel(
    tokens, gain_all, state_in_w, pool_in_w, rate_real_all, rate_imag_all, log_step_all, input_real, input_imag,
    output_real, output_imag, skip_all, pool_weight, pool_gain_all, state_out_w, pool_out_w, out,
    gain, rate_real, rate_imag, log_step, skip_gain, pool_gain, own_tokens, tok, scaled, win, wst, wpo, in_re, in_im, out_re, out_im, mix_raw,
    drive, read, unsort, bands, tails, recip, push, high, low, ends, halo, sbuf, pbuf,
    local_sem, tok_send, tok_recv, win_send, win_recv, wout_send, wout_recv,
    ready, end_send, end_recv, halo_send, halo_recv, s_send, s_recv, p_send, p_recv,
):
    s, t = lax.axis_index("sp"), lax.axis_index("tp")
    z, x, y, c = s // 4, s % 4, t // 2, t % 2
    g0 = t * GROUPS

    def lanes(ref, index, width):
        return ref.at[:, pl.ds(pl.multiple_of(index * width, 128), width)]

    def rows(ref, start, count):
        return ref.at[pl.ds(pl.multiple_of(start, 16), count), :]

    loads = [
        (tokens, own_tokens),
        (state_in_w, win.at[pl.ds(pl.multiple_of(s * 192, 16), 192), 0:128]),
        (pool_in_w, win.at[pl.ds(pl.multiple_of(s * 192, 16), 192), 128:256]),
        (state_out_w, rows(wst, s * 64, 64)),
        (pool_out_w, rows(wpo, s * 64, 64)),
        (input_real.at[pl.ds(g0, GROUPS)], in_re),
        (input_imag.at[pl.ds(g0, GROUPS)], in_im),
        (output_real.at[pl.ds(g0, GROUPS)], out_re),
        (output_imag.at[pl.ds(g0, GROUPS)], out_im),
        (pool_weight.at[pl.ds(2 * t, 2)], mix_raw),
        (gain_all, gain),
        (rate_real_all.at[pl.ds(pl.multiple_of(g0, 8), GROUPS), :], rate_real),
        (rate_imag_all.at[pl.ds(pl.multiple_of(g0, 8), GROUPS), :], rate_imag),
        (log_step_all, log_step),
        (lanes(skip_all, t, 128), skip_gain),
        (lanes(pool_gain_all, t, 128), pool_gain),
    ]
    loads = [pltpu.make_async_copy(a, b, local_sem.at[k]) for k, (a, b) in enumerate(loads)]
    for load in loads:
        load.start()

    barrier = pltpu.get_barrier_semaphore()
    beside = [z * 4 + lax.rem(x + k, 4) for k in (1, 2, 3)]
    above = [lax.rem(z + k, 4) * 4 + x for k in (1, 2, 3)]
    for peer in (*beside, *above):
        pl.semaphore_signal(barrier, inc=1, device_id={"sp": peer}, device_id_type=MESH)
    for k in range(1, HEADS_TP):
        pl.semaphore_signal(barrier, inc=1, device_id={"tp": lax.rem(t + k, HEADS_TP)}, device_id_type=MESH)

    r0, r1 = iota((ROWS, ROWS), 0), iota((ROWS, ROWS), 1)
    loads[0].wait()
    sort = (position_of(r0) == r1).astype(BF16)
    lanes(tok, t, FEATURES)[...] = dot(sort, own_tokens[...]).astype(BF16)
    unsort[...] = (position_of(r1) == r0).astype(BF16)

    def halves(ref, width, sems, across, count):
        def of(k):
            size = ROWS // count
            return lambda p: ref.at[pl.ds(k * size, size), pl.ds(pl.multiple_of(p * width, 128), width)]
        return [LineGather(of(k), sems, 3 * k, (3 * count, 3 * count + 1), y, c, across) for k in range(count)]

    tok_lines = halves(tok, FEATURES, (tok_send, tok_recv), False, 4)
    w_in = PlaneGather(
        lambda q: rows(win, q * 192, 96), lambda q: rows(win, q * 192 + 96, 96), (win_send, win_recv),
        lambda half, n: win.at[0 : 96 * n], z, x)
    w_out = PlaneGather(
        lambda q: rows(wst, q * 64, 64), lambda q: rows(wpo, q * 64, 64), (wout_send, wout_recv),
        lambda half, n: (wst, wpo)[half].at[0 : 64 * n], z, x)
    pl.semaphore_wait(barrier, 6 + HEADS_TP - 1)
    for line in tok_lines:
        line.ahead.start()
        line.back.start()
    for load in loads[1:3]:
        load.wait()
    w_in.begin()
    for line in tok_lines:
        line.own.start()
    for peer in beside:
        pl.semaphore_signal(ready, inc=1, device_id={"sp": peer}, device_id_type=MESH)
    for load in loads[3:]:
        load.wait()

    wanted = iota((GROUPS, STATE), 0) + g0
    steps_log = jnp.sum(jnp.where(iota((GROUPS, 64), 1) == wanted, log_step[...], 0.0), axis=1, keepdims=True)
    step = jnp.exp(steps_log) / float(ROWS * PEERS)
    real = rate_real[...]
    imag = rate_imag[...]
    exponent, angle = real * step, imag * step
    magnitude = jnp.exp(exponent)
    cosine, sine, half_sine = jnp.cos(angle), jnp.sin(angle), jnp.sin(0.5 * angle)
    decay_real, decay_imag = magnitude * cosine, magnitude * sine
    less = exponent * (1.0 + exponent * 0.5 * (1.0 + exponent * (1.0 / 3.0) * (1.0 + exponent * 0.25)))
    less = less * cosine - 2.0 * half_sine * half_sine
    denominator = real * real + imag * imag
    factor_real = (less * real + decay_imag * imag) / denominator
    factor_imag = (decay_imag * real - less * imag) / denominator

    spread = (iota((STATE, WIDTH), 1) % STATE == iota((STATE, WIDTH), 0)).astype(F32)
    own_group = iota((GROUPS, WIDTH), 1) // STATE == iota((GROUPS, WIDTH), 0)

    def flat(value):
        return jnp.sum(jnp.where(own_group, dot(value, spread, HIGHEST), 0.0), axis=0, keepdims=True)

    lr, li = flat(decay_real), flat(decay_imag)
    fr, fi = flat(factor_real), flat(factor_imag)

    def times(ar, ai, br, bi):
        return ar * br - ai * bi, ar * bi + ai * br

    pr, pi = lr, li
    for _ in range(5):
        pr, pi = times(pr, pi, pr, pi)
    part_real, part_imag = pr, pi
    for _ in range(3):
        pr, pi = times(pr, pi, pr, pi)
    block_real, block_imag = pr, pi
    sub = iota((PARTS, WIDTH), 0)
    up_real, up_imag = jnp.ones((PARTS, WIDTH), F32), jnp.zeros((PARTS, WIDTH), F32)
    down_real, down_imag = up_real, up_imag
    wr, wi = jnp.ones((1, WIDTH), F32), jnp.zeros((1, WIDTH), F32)
    for k in range(1, PARTS):
        wr, wi = times(wr, wi, part_real, part_imag)
        up_real, up_imag = jnp.where(sub == k, wr, up_real), jnp.where(sub == k, wi, up_imag)
        down_real = jnp.where(sub == PARTS - 1 - k, wr, down_real)
        down_imag = jnp.where(sub == PARTS - 1 - k, wi, down_imag)

    own_read = iota((128, WIDTH), 0) // CHANNEL == iota((128, WIDTH), 1) // STATE
    for k, ref in enumerate((in_re, in_im)):
        wide = jnp.where(own_read, dot(ref[...].reshape(128, STATE), spread, HIGHEST), 0.0)
        top, rest = split(wide)
        drive[0:128, k * WIDTH : (k + 1) * WIDTH] = top
        drive[128:256, k * WIDTH : (k + 1) * WIDTH] = rest
    cr = jnp.where(own_read, dot(out_re[...].reshape(128, STATE), spread, HIGHEST), 0.0)
    ci = jnp.where(own_read, dot(out_im[...].reshape(128, STATE), spread, HIGHEST), 0.0)
    for k, part in enumerate((cr * fr - ci * fi, -(cr * fi + ci * fr))):
        top, rest = split(jnp.transpose(part))
        read[k * WIDTH : (k + 1) * WIDTH, 0:128] = top
        read[k * WIDTH : (k + 1) * WIDTH, 128:256] = rest

    window0 = jnp.where(c == 0, 2, 8)
    p0, p1 = position_of(r0), position_of(r1)
    for k in range(2):
        w = window0 * (k + 1)
        bands[k * ROWS : (k + 1) * ROWS, :] = ((p1 <= p0) & (p1 > p0 - w)).astype(BF16)
        h0, h1 = position_of(iota((ROWS, REACH), 0)), iota((ROWS, REACH), 1) - REACH
        tails[k * ROWS : (k + 1) * ROWS, :] = (h1 > h0 - w).astype(BF16)
    first_head = iota((ROWS, 128), 1) < 64
    here = position_of(iota((ROWS, 128), 0)) + s * ROWS + 1
    recip[...] = 1.0 / jnp.minimum(here, jnp.where(first_head, window0, 2 * window0)).astype(F32)
    last = (position_of(iota((REACH, ROWS), 1)) == iota((REACH, ROWS), 0) + (ROWS - REACH)).astype(BF16)

    pair = (iota((64, 128), 1) % 64 == iota((64, 128), 0)).astype(BF16)
    mixer = jnp.where(
        iota((128, 128), 0) // 64 == iota((128, 128), 1) // 64, dot(mix_raw[...].reshape(128, 64), pair), 0.0
    ).astype(BF16)

    def prepare(p, squares):
        ref = lanes(tok, p, FEATURES)
        f = ref[...].astype(F32)
        lanes(scaled, p, FEATURES)[...] = (f * gain[:, pl.ds(pl.multiple_of(p * FEATURES, 128), FEATURES)]).astype(BF16)
        f = f * f
        return squares + (f[:, 0:128] + f[:, 128:256] + f[:, 256:384])

    squares = prepare(t, jnp.zeros((ROWS, 128), F32))

    def relay(line):
        line.ahead.arrive()
        line.onward.start()
        if line.across:
            line.cross_far.start()
        line.cross_ahead.start()
        line.back.arrive()
        line.cross_back.start()

    def relay_far(line):
        line.onward.arrive()
        if not line.across:
            line.cross_far.start()

    events, later = w_in.events(), w_out.events()
    one, two, three, four = tok_lines
    index = one.index

    def run(which, first, last):
        for e in which[first:last]:
            e()

    run(events, 0, 4)
    relay(one)
    run(events, 4, 6)
    relay(two)
    run(events, 6, 8)
    relay(three)
    relay(four)
    run(events, 8, 14)
    w_out.begin()
    for line in (one, two, three):
        relay_far(line)
    for name in ("ahead", "back"):
        squares = prepare(index[name], squares)
    relay_far(four)
    squares = prepare(index["onward"], squares)
    one.own.arrive_all(tok.at[:, 0 : 3 * FEATURES])
    for name in ("p_own", "p_ahead", "p_back"):
        squares = prepare(index[name], squares)
    one.cross_far.arrive_all(tok.at[:, 0:FEATURES])
    squares = prepare(index["p_onward"], squares)
    inverse = lax.rsqrt(jnp.sum(squares, axis=1, keepdims=True) / 3072.0 + EPSILON)

    def row_part(ref, dz, width, axis):
        at = pl.ds(pl.multiple_of(lax.rem(z + dz + 4, 4) * width, 128), width)
        return ref[:, at] if axis else ref[at, :]

    product = jnp.zeros((ROWS, 256), F32)
    for dz in (0, 1, -1, 2):
        w_in.ready(dz)
        product = product + dot(row_part(scaled, dz, 768, 1), row_part(win, dz, 768, 0))
    entry = (product * inverse).astype(BF16)
    state_in, pool_in = entry[:, 0:128], entry[:, 128:256]

    pl.semaphore_wait(ready, 3)
    halo[s] = dot(last, pool_in).astype(BF16)
    back = lax.rem(s + PEERS - 1, PEERS)
    halo_move = Move(halo.at[s], halo.at[back], {"sp": lax.rem(s + 1, PEERS)}, halo_send.at[0], halo_recv.at[0])
    halo_move.start()

    push[...] = dot(jnp.concatenate([state_in, state_in], axis=1), drive[...])
    lrb, lib = jnp.broadcast_to(lr, (PARTS, WIDTH)), jnp.broadcast_to(li, (PARTS, WIDTH))

    def advance(j, carry):
        sr, si = carry
        at = pl.ds(pl.multiple_of(j * PARTS, PARTS), PARTS)
        nr = lrb * sr - lib * si + push[at, 0:WIDTH]
        ni = lrb * si + lib * sr + push[at, WIDTH : 2 * WIDTH]
        return nr, ni

    zero = jnp.zeros((PARTS, WIDTH), F32)
    er, ei = lax.fori_loop(0, STEPS, advance, (zero, zero), unroll=8)
    br, bi = times(er, ei, down_real, down_imag)
    br, bi = jnp.sum(br, axis=0, keepdims=True), jnp.sum(bi, axis=0, keepdims=True)
    lines = lambda row: [row[:, 128 * k : 128 * (k + 1)] for k in range(WIDTH // 128)]
    ends[s] = jnp.concatenate(lines(br) + lines(bi), axis=0)
    block = lambda dz, dx: lax.rem(z + dz + 4, 4) * 4 + lax.rem(x + dx + 4, 4)
    offsets = [(dz, dx) for dz in (2, 1, -1, 0) for dx in (2, 1, -1, 0)][:-1]
    farthest_first = sorted(offsets, key=lambda o: -abs(o[0]) - abs(o[1]))
    moves = [
        Move(ends.at[s], ends.at[block(-dz, -dx)], {"sp": block(dz, dx)}, end_send.at[0], end_recv.at[0])
        for dz, dx in farthest_first
    ]
    for m in moves:
        m.start()

    sums = dot(bands[...], pool_in)
    halo_move.arrive()
    before = halo[back]
    before = jnp.where(s > 0, before.astype(F32), 0.0).astype(BF16)
    sums = sums + dot(tails[...], before)
    pooled = jnp.where(first_head, sums[0:ROWS], sums[ROWS : 2 * ROWS]) * recip[...] - pool_in.astype(F32)
    top, rest = split(pooled)
    projected = dot(top, mixer) + dot(rest, mixer)
    pool_out = (projected * pool_gain[...]).astype(BF16)
    lanes(pbuf, t, 128)[...] = dot(unsort[...], pool_out).astype(BF16)
    pline = LineGather(lambda p: lanes(pbuf, p, 128), (p_send, p_recv), 0, (3, 3), y, c, True)
    pline.ahead.start()
    pline.back.start()
    pline.own.start()

    kr, ki = jnp.where(sub >= 1, pltpu.roll(er, 1, 0), 0.0), jnp.where(sub >= 1, pltpu.roll(ei, 1, 0), 0.0)
    gr, gi = part_real, part_imag
    for hop in (1, 2, 4):
        tr = jnp.where(sub >= hop, pltpu.roll(kr, hop, 0), 0.0)
        ti = jnp.where(sub >= hop, pltpu.roll(ki, hop, 0), 0.0)
        ar, ai = times(tr, ti, gr, gi)
        kr, ki = kr + ar, ki + ai
        gr, gi = times(gr, gi, gr, gi)

    run(later, 0, 6)
    moves[0].arrive_all(ends.at[0 : PEERS - 1])
    qr = jnp.concatenate(lines(block_real), axis=0)
    qi = jnp.concatenate(lines(block_imag), axis=0)
    hr, hi = jnp.zeros_like(qr), jnp.zeros_like(qi)
    for q in range(PEERS - 1):
        piece = ends[q]
        ar, ai = times(hr, hi, qr, qi)
        hr, hi = jnp.where(q < s, ar + piece[0:4], hr), jnp.where(q < s, ai + piece[4:8], hi)
    hr = jnp.concatenate([hr[k : k + 1] for k in range(4)], axis=1)
    hi = jnp.concatenate([hi[k : k + 1] for k in range(4)], axis=1)
    ar, ai = times(up_real, up_imag, hr, hi)

    def advance_pair(j, carry):
        one = advance(2 * j, carry)
        two = advance(2 * j + 1, one)
        at = pl.ds(pl.multiple_of(j * 2 * PARTS, 2 * PARTS), 2 * PARTS)
        for k in range(2):
            top, rest = split(jnp.concatenate([one[k], two[k]], axis=0))
            high[at, k * WIDTH : (k + 1) * WIDTH] = top
            low[at, k * WIDTH : (k + 1) * WIDTH] = rest
        return two

    lax.fori_loop(0, STEPS // 2, advance_pair, (kr + ar, ki + ai), unroll=4)
    both = dot(high[...], read[...])
    readout = both[:, 0:128] + both[:, 128:256] + dot(low[...], read[:, 0:128])
    readout = readout + skip_gain[...] * state_in.astype(F32)
    state_out = jax.nn.gelu(readout).astype(BF16)
    lanes(sbuf, t, 128)[...] = dot(unsort[...], state_out).astype(BF16)
    s_lines = halves(sbuf, 128, (s_send, s_recv), True, 2)
    for line in s_lines:
        line.ahead.start()
        line.back.start()
    for line in s_lines:
        line.own.start()
    relay(pline)
    for line in s_lines:
        relay(line)
    run(later, 6, 14)
    relay_far(pline)
    pline.own.arrive_all(pbuf.at[:, 0:512])
    total = jnp.zeros((ROWS, FEATURES), F32)
    for dz in (0, 1, -1):
        w_out.ready(dz)
        total = total + dot(row_part(pbuf, dz, 256, 1), row_part(wpo, dz, 256, 0))
    for line in s_lines:
        relay_far(line)
    s_lines[0].own.arrive_all(sbuf.at[:, 0 : 3 * 128])
    s_lines[0].cross_far.arrive_all(sbuf.at[:, 0:128])
    for dz in (0, 1, -1):
        total = total + dot(row_part(sbuf, dz, 256, 1), row_part(wst, dz, 256, 0))
    w_out.ready(2)
    total = total + dot(row_part(pbuf, 2, 256, 1), row_part(wpo, 2, 256, 0))
    total = total + dot(row_part(sbuf, 2, 256, 1), row_part(wst, 2, 256, 0))
    out[...] = total.astype(BF16)

    one.own.left_all(tok.at[:, 0 : 7 * FEATURES])
    for plane, refs in ((w_in, (win.at[0:1440], win.at[0:1440])), (w_out, (wst.at[0:960], wpo.at[0:960]))):
        plane.a[0].left_all(refs[0])
        plane.b[0].left_all(refs[1])
    moves[0].left_all(ends.at[0 : PEERS - 1])
    pline.own.left_all(pbuf.at[:, 0:896])
    s_lines[0].own.left_all(sbuf.at[:, 0:896])
    halo_move.left_all(halo.at[0])


def body(
    tokens, norm_gain, state_in_weight, pool_in_weight, rate_real, rate_imag, log_step, input_real, input_imag,
    output_real, output_imag, skip_gain, pool_weight, pool_gain, state_out_weight, pool_out_weight,
):
    vmem = pl.BlockSpec(memory_space=pltpu.VMEM)
    dma = pltpu.SemaphoreType.DMA
    return pl.pallas_call(
        kernel,
        out_shape=pltpu.VMEM((ROWS, FEATURES), BF16),
        in_specs=[pl.BlockSpec(memory_space=pltpu.HBM)] * 16,
        out_specs=vmem,
        scratch_shapes=[
            pltpu.VMEM((1, 3072), F32),
            pltpu.VMEM((GROUPS, STATE), F32),
            pltpu.VMEM((GROUPS, STATE), F32),
            pltpu.VMEM((1, 64), F32),
            pltpu.VMEM((1, 128), F32),
            pltpu.VMEM((1, 128), F32),
            pltpu.VMEM((ROWS, FEATURES), BF16),
            pltpu.VMEM((ROWS, 3072), BF16),
            pltpu.VMEM((ROWS, 3072), BF16),
            pltpu.VMEM((3072, 256), BF16),
            pltpu.VMEM((1024, FEATURES), BF16),
            pltpu.VMEM((1024, FEATURES), BF16),
            pltpu.VMEM((GROUPS, CHANNEL, STATE), F32),
            pltpu.VMEM((GROUPS, CHANNEL, STATE), F32),
            pltpu.VMEM((GROUPS, CHANNEL, STATE), F32),
            pltpu.VMEM((GROUPS, CHANNEL, STATE), F32),
            pltpu.VMEM((2, 64, 64), BF16),
            pltpu.VMEM((256, 2 * WIDTH), BF16),
            pltpu.VMEM((2 * WIDTH, 256), BF16),
            pltpu.VMEM((ROWS, ROWS), BF16),
            pltpu.VMEM((2 * ROWS, ROWS), BF16),
            pltpu.VMEM((2 * ROWS, REACH), BF16),
            pltpu.VMEM((ROWS, 128), F32),
            pltpu.VMEM((ROWS, 2 * WIDTH), F32),
            pltpu.VMEM((ROWS, 2 * WIDTH), BF16),
            pltpu.VMEM((ROWS, 2 * WIDTH), BF16),
            pltpu.VMEM((PEERS, 8, 128), F32),
            pltpu.VMEM((PEERS, REACH, 128), BF16),
            pltpu.VMEM((ROWS, 1024), BF16),
            pltpu.VMEM((ROWS, 1024), BF16),
            dma((16,)), dma((1,)), dma((16,)), dma((2,)), dma((24,)), dma((2,)), dma((24,)),
            pltpu.SemaphoreType.REGULAR, dma((1,)), dma((1,)), dma((1,)), dma((1,)),
            dma((1,)), dma((8,)), dma((1,)), dma((4,)),
        ],
        compiler_params=pltpu.CompilerParams(collective_id=0, has_side_effects=True, vmem_limit_bytes=60000000),
    )(*(pltpu.with_memory_space_constraint(v, pltpu.HBM) for v in (
        tokens, norm_gain.reshape(1, 3072), state_in_weight, pool_in_weight, rate_real, rate_imag,
        log_step.reshape(1, 64), jnp.swapaxes(input_real, 1, 2), jnp.swapaxes(input_imag, 1, 2), output_real, output_imag, skip_gain.reshape(1, 1024),
        pool_weight, pool_gain.reshape(1, 1024), state_out_weight, pool_out_weight,
    )))


def solution(mesh):
    tile = P("sp", "tp")
    in_specs = (tile, P(), tile, tile, *(P() for _ in range(10)), tile, tile)
    return jax.shard_map(body, mesh=mesh, in_specs=in_specs, out_specs=tile, check_vma=False)
```
